32 devices in a mesh: grp: 2 (over y), sp: 4 (over z), tp: 4 (over x, core).
Axes of the slice: x: 2, y: 2, z: 4, core: 2. Of those that a mesh axis runs over, the one named last changes fastest.
Arguments:
- target: bfloat16 [1024, 2048], P(('grp', 'sp', 'tp')), parts along dimension 0, may hold values from -5 to 5
- source: bfloat16 [8192, 2048], P(('grp', 'sp', 'tp')), parts along dimension 0, may hold values from -5 to 5
- source_gain: float32 [2048], replicated, may hold values from 0.1 to 1.9
- pre_first: float32 [2048], replicated, may hold values from 0.1 to 1.9
- query_first: bfloat16 [2048, 2048], P(None, 'tp')
- keyval_first: bfloat16 [2048, 1024], P(None, 'tp')
- out_first: bfloat16 [2048, 2048], P('tp'), may hold values from -0.125 to 0.125
- post_first: float32 [2048], replicated, may hold values from 0.1 to 1.9
- ffn_pre: float32 [2048], replicated, may hold values from 0.1 to 1.9
- w_gate: bfloat16 [2048, 2816], P(None, 'tp'), may hold values from -0.125 to 0.125
- w_value: bfloat16 [2048, 2816], P(None, 'tp'), may hold values from -0.125 to 0.125
- conv_gate: float32 [3, 2816], P(None, 'tp'), may hold values from -3.5 to 3.5
- conv_value: float32 [3, 2816], P(None, 'tp'), may hold values from -3.5 to 3.5
- w_down: bfloat16 [2816, 2048], P('tp'), may hold values from -0.109375 to 0.109375
- ffn_post: float32 [2048], replicated, may hold values from 0.1 to 1.9
- pre_second: float32 [2048], replicated, may hold values from 0.1 to 1.9
- query_second: bfloat16 [2048, 2048], P(None, 'tp')
- keyval_second: bfloat16 [2048, 1024], P(None, 'tp')
- out_second: bfloat16 [2048, 2048], P('tp'), may hold values from -0.125 to 0.125
- post_second: float32 [2048], replicated, may hold values from 0.1 to 1.9
Outputs:
- decoded: float32 [1024, 2048], P(('grp', 'sp', 'tp')), parts along dimension 0
The draws below stay inside these ranges and needn't reach their ends.
There are 2 independent parts, one for each index of `grp`. The reference program is written for one: setup_inputs(seed, part) draws one part's arguments, and reference() takes and returns one part's arrays. A program takes and returns all parts, laid end to end along the dimension named above; an argument that names none is the same for every part. Nothing has to cross between parts.
All inputs are finite; a program needn't handle non-finite values.
Results may differ from the reference program's by a relative error of at most 0.04.
Values may be sent and summed in bfloat16 or wider, within the bound.
A program may use at most 128 MiB of HBM per device.

```python
import jax
import jax.numpy as jnp
from jax import lax

D = 2048
HEAD = 128
QH = 16
KVH = 4
FF = 2816
TARGET = 512
SOURCE = 4096
N_TP = 4


def draw_target(key, part):
    rows = jnp.clip(jax.random.normal(jax.random.fold_in(key, 11), (TARGET, D), jnp.float32), -5.0, 5.0)
    return rows.astype(jnp.bfloat16)


def draw_source(key, part):
    rows = jnp.clip(jax.random.normal(jax.random.fold_in(key, 12), (SOURCE, D), jnp.float32), -5.0, 5.0)
    return rows.astype(jnp.bfloat16)


def layer_weights(key, salt):
    drawn_query = jax.random.normal(jax.random.fold_in(key, salt + 1), (D, QH * HEAD), jnp.float32) * D ** (-0.5)
    drawn_keyval = jax.random.normal(jax.random.fold_in(key, salt + 2), (D, KVH, 2, HEAD), jnp.float32) * D ** (-0.5)
    return (drawn_query, drawn_keyval.reshape(D, KVH * 2 * HEAD))


def draw_query_first(key, part):
    return layer_weights(key, 41)[0].astype(jnp.bfloat16)


def draw_keyval_first(key, part):
    return layer_weights(key, 41)[1].astype(jnp.bfloat16)


def draw_query_second(key, part):
    return layer_weights(key, 51)[0].astype(jnp.bfloat16)


def draw_keyval_second(key, part):
    return layer_weights(key, 51)[1].astype(jnp.bfloat16)


def block_levels(stream_key, dims, cuts, smallest, top_value):
    loudness, own = 1.0, jax.random.fold_in(stream_key, 6)
    for dim, shards_of in cuts:
        draws = jnp.exp(jax.random.uniform(jax.random.fold_in(own, dim), (shards_of,), jnp.float32, smallest / len(cuts), top_value / len(cuts)))
        loudness = loudness * jnp.repeat(draws, dims[dim] // shards_of).reshape([-1 if axis == dim else 1 for axis in range(len(dims))])
    return loudness


def bell_draw(own_key, shape, scale, bound, split=(), held_as=jnp.bfloat16):
    result = jax.random.normal(own_key, shape, jnp.float32) * scale
    if len(split) > 0:
        result = block_levels(own_key, shape, split, -0.22, 0.18) * result
    return jnp.clip(result, min=-bound, max=bound).astype(held_as)


def setup_inputs(seed: int = 0, part: int = 0) -> dict:
    key_of = jax.random.split(jax.random.key(seed), 21)
    part_splits = jax.random.split(jax.random.fold_in(key_of[20], part), 21)
    return {
        "target": draw_target(jax.random.fold_in(jax.random.fold_in(key_of[20], part), 71), part),
        "source": draw_source(jax.random.fold_in(jax.random.fold_in(key_of[20], part), 71), part),
        "source_gain": jnp.clip(jax.random.uniform(key_of[2], (D,), jnp.float32, 0.1, 1.9), 0.1, 1.9),
        "pre_first": jnp.clip(jax.random.uniform(key_of[3], (D,), jnp.float32, 0.1, 1.9), 0.1, 1.9),
        "query_first": draw_query_first(jax.random.fold_in(key_of[20], 71), part),
        "keyval_first": draw_keyval_first(jax.random.fold_in(key_of[20], 71), part),
        "out_first": bell_draw(key_of[6], (QH * HEAD, D), (QH * HEAD) ** -0.5, 0.125, ((0, 4),)),
        "post_first": jnp.clip(jax.random.uniform(key_of[7], (D,), jnp.float32, 0.1, 1.9), 0.1, 1.9),
        "ffn_pre": jnp.clip(jax.random.uniform(key_of[8], (D,), jnp.float32, 0.1, 1.9), 0.1, 1.9),
        "w_gate": bell_draw(key_of[9], (D, FF), D ** -0.5, 0.125, ((1, 4),)),
        "w_value": bell_draw(key_of[10], (D, FF), D ** -0.5, 0.125, ((1, 4),)),
        "conv_gate": bell_draw(key_of[11], (3, FF), 3 ** -0.5, 3.5, ((1, 4),), jnp.float32),
        "conv_value": bell_draw(key_of[12], (3, FF), 3 ** -0.5, 3.5, ((1, 4),), jnp.float32),
        "w_down": bell_draw(key_of[13], (FF, D), FF ** -0.5, 0.109375, ((0, 4),)),
        "ffn_post": jnp.clip(jax.random.uniform(key_of[14], (D,), jnp.float32, 0.1, 1.9), 0.1, 1.9),
        "pre_second": jnp.clip(jax.random.uniform(key_of[15], (D,), jnp.float32, 0.1, 1.9), 0.1, 1.9),
        "query_second": draw_query_second(jax.random.fold_in(key_of[20], 71), part),
        "keyval_second": draw_keyval_second(jax.random.fold_in(key_of[20], 71), part),
        "out_second": bell_draw(key_of[18], (QH * HEAD, D), (QH * HEAD) ** -0.5, 0.125, ((0, 4),)),
        "post_second": jnp.clip(jax.random.uniform(key_of[19], (D,), jnp.float32, 0.1, 1.9), 0.1, 1.9),
    }


def normed(values, gain):
    widened = values.astype(jnp.float32)
    return widened * lax.rsqrt(lax.optimization_barrier(jnp.mean(widened * widened, axis=-1, keepdims=True)) + 1e-06) * gain

def sharded_product(left_side, right_side, shards):
    column_span = left_side.shape[1] // shards

    def accumulate(running, shard_index):
        left_part = lax.dynamic_slice_in_dim(left_side, shard_index * column_span, column_span, 1)
        right_part = lax.dynamic_slice_in_dim(right_side, shard_index * column_span, column_span, 0)
        rounded = jnp.dot(left_part, right_part, preferred_element_type=jnp.float32).astype(jnp.bfloat16)
        rounded = lax.optimization_barrier(rounded)
        return (running + rounded.astype(jnp.float32), None)
    initial = jnp.zeros((left_side.shape[0], right_side.shape[1]), jnp.float32)
    summed, unused = lax.scan(accumulate, initial, jnp.arange(shards, dtype=jnp.int32))
    return summed

def attend(queries, keyvals):
    group_size = QH // KVH
    scale_factor = HEAD ** (-0.5)
    query_heads = jnp.moveaxis(queries.reshape(TARGET, QH, HEAD), 1, 0)

    def one_head(inputs):
        head_queries, head_index = inputs
        columns = lax.dynamic_slice_in_dim(keyvals, head_index // group_size * (2 * HEAD), 2 * HEAD, 1)
        head_keys = columns[:, :HEAD]
        head_values = columns[:, HEAD:]
        scores = lax.dot_general(head_queries, head_keys, (((1,), (1,)), ((), ())), preferred_element_type=jnp.float32) * scale_factor
        row_max = lax.optimization_barrier(jnp.max(scores, axis=1, keepdims=True))
        weights = jnp.exp(scores - row_max)
        weight_sum = lax.optimization_barrier(jnp.sum(weights, axis=1, keepdims=True))
        gathered = jnp.dot(weights.astype(jnp.bfloat16), head_values, preferred_element_type=jnp.float32)
        return (gathered / weight_sum).astype(jnp.bfloat16)
    outputs = lax.map(one_head, (query_heads, jnp.arange(QH, dtype=jnp.int32)))
    return jnp.moveaxis(outputs, 0, 1).reshape(TARGET, QH * HEAD)

def attention_layer(stream, pre_gain, w_query, keyvals, w_out, post_gain):
    hidden = normed(stream, pre_gain).astype(jnp.bfloat16)
    queries = jnp.dot(hidden, w_query, preferred_element_type=jnp.float32).astype(jnp.bfloat16)
    heads = attend(queries, keyvals)
    mixed = sharded_product(heads, w_out, N_TP)
    return stream.astype(jnp.float32) + normed(mixed, post_gain)

def causal_mix(up_rows, conv_taps):
    padded = jnp.pad(up_rows.astype(jnp.float32), ((2, 0), (0, 0)))
    length = up_rows.shape[0]
    return conv_taps[0] * padded[:length] + conv_taps[1] * padded[1:length + 1] + conv_taps[2] * padded[2:]

def reference(target, source, source_gain, pre_first, query_first, keyval_first, out_first, post_first, ffn_pre, w_gate, w_value, conv_gate, conv_value, w_down, ffn_post, pre_second, query_second, keyval_second, out_second, post_second):
    source_normed = normed(source, source_gain).astype(jnp.bfloat16)
    kv_first = jnp.dot(source_normed, keyval_first, preferred_element_type=jnp.float32).astype(jnp.bfloat16)
    kv_second = jnp.dot(source_normed, keyval_second, preferred_element_type=jnp.float32).astype(jnp.bfloat16)
    after_first = attention_layer(target, pre_first, query_first, kv_first, out_first, post_first)
    ffn_input = normed(after_first, ffn_pre).astype(jnp.bfloat16)
    up_gate = jnp.dot(ffn_input, w_gate, preferred_element_type=jnp.float32).astype(jnp.bfloat16)
    up_value = jnp.dot(ffn_input, w_value, preferred_element_type=jnp.float32).astype(jnp.bfloat16)
    gated = (jax.nn.gelu(causal_mix(up_gate, conv_gate), approximate=True) * causal_mix(up_value, conv_value)).astype(jnp.bfloat16)
    ffn_sum = sharded_product(gated, w_down, N_TP)
    after_ffn = after_first + normed(ffn_sum, ffn_post)
    return attention_layer(after_ffn, pre_second, query_second, kv_second, out_second, post_second)
```

```python
import math

import jax
import jax.numpy as jnp
from jax import lax
from jax.experimental import pallas as pl
from jax.experimental.pallas import tpu as pltpu
from jax.sharding import PartitionSpec as P

HEAD = 128
CHUNKS = 4
PIECES = 2
EXP_SCALE = HEAD ** (-0.5) * math.log2(math.e)
F32, BF16 = jnp.float32, jnp.bfloat16
MESH = pl.DeviceIdType.MESH


def normed(values, gain):
    widened = values.astype(F32)
    return widened * lax.rsqrt(jnp.mean(widened * widened, axis=-1, keepdims=True) + 1e-06) * gain


SC = jax.named_scope


def times(start, stop, body):
    if stop - start <= 4:
        for index in range(start, stop):
            body(index)
    else:

        @pl.loop(start, stop)
        def _(index):
            body(index)


def dot(left, right):
    return jnp.dot(left, right, preferred_element_type=F32)


def decoder_kernel(
    n_tp,
    n_sp,
    target_h,
    source_h,
    source_gain,
    pre_first,
    query_first_h,
    keyval_first_h,
    out_first_h,
    post_first,
    ffn_pre,
    gate_h,
    value_h,
    conv_gate,
    conv_value,
    down_h,
    ffn_post,
    pre_second,
    query_second_h,
    keyval_second_h,
    out_second_h,
    post_second,
    decoded,
    target_v,
    source_v,
    query_first,
    keyval_first,
    out_first,
    gate_t,
    value_t,
    w_gate,
    w_value,
    w_down,
    query_second,
    keyval_second,
    out_second,
    local_sem,
    hidden,
    hidden_send,
    hidden_recv,
    src,
    src_send,
    src_recv,
    q_slots,
    q_sem,
    k_first,
    v_first,
    k_second,
    v_second,
    kv_send,
    kv_recv,
    run_max,
    run_sum,
    run_out,
    mix_send,
    mix_recv,
    stat_send,
    stat_recv,
    mix_sem,
    part,
    pair_recv,
    pair_sum,
    part_recv,
    part_send,
    pair_sem,
    part_sem,
    halo_send,
    halo_recv,
    halo_sem,
    stream,
):
    me = lax.axis_index("tp")
    z = lax.axis_index("sp")
    sib = me + 1 - 2 * lax.rem(me, 2)
    core, chip = lax.rem(me, 2), me // 2
    n_chip = n_tp // 2
    rows = target_v.shape[0]
    width = target_v.shape[1]
    span = width // PIECES
    chunk = src.shape[2]
    block_rows = rows * n_tp

    def tp_at(distance):
        return lax.rem(me + distance, n_tp)

    def sp_at(distance):
        return lax.rem(z + distance, n_sp)

    def to_tp(source, dest, send, recv, device):
        return pltpu.make_async_remote_copy(
            src_ref=source, dst_ref=dest, send_sem=send, recv_sem=recv,
            device_id={"tp": device}, device_id_type=MESH,
        )

    def to_sp(source, dest, send, recv, device):
        return pltpu.make_async_remote_copy(
            src_ref=source, dst_ref=dest, send_sem=send, recv_sem=recv,
            device_id={"sp": device}, device_id_type=MESH,
        )

    pairs = [
        (target_h, target_v),
        (source_h, source_v),
        (query_first_h, query_first),
        (keyval_first_h, keyval_first),
        (keyval_second_h, keyval_second),
        (out_first_h, out_first),
        (gate_h, gate_t),
        (value_h, value_t),
        (down_h, w_down),
        (query_second_h, query_second),
        (out_second_h, out_second),
    ]
    loads = [
        pltpu.make_async_copy(a, b, local_sem.at[i]) for i, (a, b) in enumerate(pairs)
    ]
    for load in loads:
        load.start()

    barrier = pltpu.get_barrier_semaphore()
    for distance in range(1, n_tp):
        pl.semaphore_signal(barrier, inc=1, device_id={"tp": tp_at(distance)}, device_id_type=MESH)
    for distance in range(1, n_sp):
        pl.semaphore_signal(barrier, inc=1, device_id={"sp": sp_at(distance)}, device_id_type=MESH)
    last_tp = n_tp - 1

    @pl.when(jnp.logical_and(z > 0, me < last_tp))
    def _():
        pl.semaphore_signal(
            barrier, inc=1, device_id={"sp": z - 1, "tp": last_tp}, device_id_type=MESH
        )

    gives_halo = jnp.logical_and(me == last_tp, z < n_sp - 1)
    with SC("barrier"):
        pl.semaphore_wait(barrier, n_tp - 1 + n_sp - 1 + jnp.where(gives_halo, n_tp - 1, 0))

    def hidden_copy(phase, piece, slot, device):
        return to_tp(
            hidden.at[phase, piece, slot], hidden.at[phase, piece, slot],
            hidden_send.at[phase], hidden_recv.at[phase, piece, slot], device,
        )

    def gather_start(phase, value):
        for piece in range(PIECES):
            hidden[phase, piece, me] = value[:, piece * span : (piece + 1) * span].astype(BF16)
            for d in range(1, n_chip):
                hidden_copy(phase, piece, me, tp_at(2 * d)).start()
            hidden_copy(phase, piece, me, sib).start()

    def gather_times(phase, weights, extra=None):
        totals = [None] * len(weights)
        for piece in range(PIECES + 1):
            if piece < PIECES:
                for d in range(1, n_chip):
                    slot = tp_at(2 * d)
                    hidden_copy(phase, piece, slot, sib).wait_recv()
                    hidden_copy(phase, piece, slot, sib).start()
            if piece == 0:
                continue
            ready = piece - 1
            for d in range(n_chip):
                slot = lax.rem(sib + 2 * d, n_tp)
                hidden_copy(phase, ready, slot, sib).wait_recv()
            whole = hidden[phase, ready]
            if rows % 16:
                whole = whole.astype(F32).reshape(block_rows, span).astype(BF16)
            else:
                whole = whole.reshape(block_rows, span)
            if extra is not None:
                if ready == 0:
                    rim = extra()
                whole = jnp.concatenate([whole, rim[:, ready * span : (ready + 1) * span]], axis=0)
            for index, weight in enumerate(weights):
                product = dot(whole, weight[ready * span : (ready + 1) * span, :])
                totals[index] = product if ready == 0 else totals[index] + product
        return totals

    def gather_drain(phase):
        for piece in range(PIECES):
            for _ in range(2 * n_chip - 1):
                hidden_copy(phase, piece, me, sib).wait_send()

    def pair_copy(phase, piece):
        return to_tp(
            part.at[phase, piece, 1 - core], pair_recv.at[phase, piece],
            part_send.at[phase, 0], pair_sem.at[phase, piece], sib,
        )

    def chip_copy(phase, piece, distance, slot):
        other = lax.rem(chip + distance, n_chip)
        return to_tp(
            pair_sum.at[phase, piece, other], part_recv.at[phase, piece, slot],
            part_send.at[phase, 1], part_sem.at[phase, piece, slot], 2 * other + core,
        )

    def scatter_sum(phase, left, weight):
        for piece in range(PIECES):
            product = dot(left, weight[:, piece * span : (piece + 1) * span])
            product = product.reshape(n_chip, 2, rows, span)
            for parity in range(2):
                part[phase, piece, parity] = product[:, parity].astype(BF16)
            pair_copy(phase, piece).start()
        for piece in range(PIECES):
            pair_copy(phase, piece).wait_recv()
            mine = part[phase, piece, core].astype(F32)
            pair_sum[phase, piece] = (mine + pair_recv[phase, piece].astype(F32)).astype(BF16)
            for d in range(1, n_chip):
                chip_copy(phase, piece, d, chip).start()
        sums = []
        for piece in range(PIECES):
            total = pair_sum[phase, piece, chip].astype(F32)
            for d in range(1, n_chip):
                slot = lax.rem(chip + d, n_chip)
                chip_copy(phase, piece, d, slot).wait_recv()
                total = total + part_recv[phase, piece, slot].astype(F32)
            sums.append(total)
        return jnp.concatenate(sums, axis=1)

    def sum_drain(phase):
        for piece in range(PIECES):
            pair_copy(phase, piece).wait_send()
            for d in range(1, n_chip):
                chip_copy(phase, piece, d, chip).wait_send()

    def head_columns(queries):
        blocks = [
            queries[:, h : h + HEAD].T for h in range(0, queries.shape[1], HEAD)
        ]
        return jnp.concatenate(blocks, axis=1).astype(BF16)

    def head_rows(columns):
        blocks = [
            columns[:, c : c + block_rows].T for c in range(0, columns.shape[1], block_rows)
        ]
        return jnp.concatenate(blocks, axis=1).astype(BF16)

    loads[0].wait()
    with SC("norm0"):
        gather_start(0, normed(target_v[...], pre_first[...]))

    def src_copy(slot, c, device, kind):
        return to_tp(
            src.at[slot, c], src.at[slot, c], src_send.at[kind], src_recv.at[slot, c], device
        )

    loads[1].wait()
    for c in range(CHUNKS):
        src[me, c] = normed(source_v[pl.ds(c * chunk, chunk)], source_gain[...]).astype(BF16)
        for d in range(1, n_chip):
            src_copy(me, c, tp_at(2 * d), 0).start()
        src_copy(me, c, sib, 0).start()

    loads[2].wait()
    with SC("qproj"):
        q_slots[z] = head_columns(gather_times(0, [query_first])[0])

    def q_copy(distance, slot):
        return to_sp(
            q_slots.at[z], q_slots.at[z] if slot is None else q_slots.at[slot],
            q_sem.at[0, 0], q_sem.at[1, z if slot is None else slot], sp_at(distance),
        )

    for d in range(1, n_sp):
        q_copy(d, None).start()

    loads[3].wait()
    loads[4].wait()

    def project_pair(block, c, mine, other, layers=(0, 1)):
        lines = jnp.concatenate([src[mine, c], src[other, c]], axis=0)
        place = pl.ds(c * 2 * chunk, 2 * chunk)
        if 0 in layers:
            first = dot(lines, keyval_first[...])
            k_first[block, place] = first[:, :HEAD].astype(BF16)
            v_first[block, place] = first[:, HEAD:].astype(BF16)
        if 1 in layers:
            second = dot(lines, keyval_second[...])
            k_second[z, block, place] = second[:, :HEAD].astype(BF16)
            v_second[z, block, place] = second[:, HEAD:].astype(BF16)

    def absorb(keys, values, queries, slot, fresh):
        scores = dot(keys, queries)
        newest = jnp.max(scores, axis=0, keepdims=True)
        if not fresh:
            newest = jnp.maximum(newest, run_max[slot])
        weights = jnp.exp2((scores - newest) * EXP_SCALE)
        added = jnp.sum(weights, axis=0, keepdims=True)
        gathered = lax.dot_general(
            values, weights.astype(BF16), (((0,), (0,)), ((), ())), preferred_element_type=F32
        )
        if not fresh:
            rescale = jnp.exp2((run_max[slot] - newest) * EXP_SCALE)
            added = added + run_sum[slot] * rescale
            gathered = gathered + run_out[slot] * rescale
        run_max[slot] = newest
        run_sum[slot] = added
        run_out[slot] = gathered

    def absorb_block(block, fresh):
        @pl.loop(0, n_sp)
        def _(slot):
            absorb(k_first[block], v_first[block], q_slots[slot], slot, fresh)

    def kv_copies(block, slot, peer):
        return [
            to_sp(
                store.at[slot, block], store.at[slot, block],
                kv_send.at[index], kv_recv.at[index, slot, block], peer,
            )
            for index, store in enumerate((k_second, v_second))
        ]

    def kv_hop(block, hop, arrive=True, leave=True):
        for step in (1, -1):
            slot = z - step * (hop - 1)
            peer = z + step

            @pl.when(jnp.logical_and(slot >= 0, slot < n_sp))
            def _():
                if arrive:
                    for copy in kv_copies(block, slot, sp_at(1)):
                        copy.wait_recv()
                if leave:

                    @pl.when(jnp.logical_and(hop < n_sp, jnp.logical_and(peer >= 0, peer < n_sp)))
                    def _():
                        for copy in kv_copies(block, slot, peer):
                            copy.start()

    def kv_drain(block, hop):
        for step in (1, -1):
            slot = z - step * (hop - 1)
            peer = z + step
            inside = jnp.logical_and(slot >= 0, slot < n_sp)

            @pl.when(jnp.logical_and(inside, jnp.logical_and(peer >= 0, peer < n_sp)))
            def _():
                for copy in kv_copies(block, slot, peer):
                    copy.wait_send()

    for c in range(CHUNKS):
        src_copy(sib, c, sib, 0).wait_recv()
        project_pair(0, c, me, sib)
    for d in range(1, n_sp):
        q_copy(d, sp_at(d)).wait_recv()
    kv_hop(0, 1, arrive=False)
    with SC("abs_own"):
        absorb_block(0, True)

    def far_chunk(d, c, layers=(0, 1)):
        near = tp_at(2 * d)
        far = lax.rem(sib + 2 * d, n_tp)
        src_copy(near, c, sib, 1).wait_recv()
        src_copy(near, c, sib, 1).start()
        src_copy(far, c, sib, 1).wait_recv()
        project_pair(d, c, near, far, layers)

    def far_absorb(d):
        for c in range(CHUNKS):
            far_chunk(d, c)
        absorb_block(d, False)

    times(1, n_chip - 1, far_absorb)
    last = n_chip - 1
    early = (CHUNKS - 1) * 2 * chunk
    with SC("far_early"):
        for c in range(CHUNKS - 1):
            far_chunk(last, c)

    with SC("abs_early"):
        @pl.loop(0, n_sp)
        def _(slot):
            absorb(k_first[last, :early], v_first[last, :early], q_slots[slot], slot, False)

    with SC("far_last"):
        far_chunk(last, CHUNKS - 1, (0,))

    def mix_copies(distance, slot):
        peer = sp_at(distance)
        return [
            to_sp(sent.at[peer], got.at[slot], mix_sem.at[index, 0, 0], mix_sem.at[index, 1, slot], peer)
            for index, (sent, got) in enumerate(((mix_send, mix_recv), (stat_send, stat_recv)))
        ]

    def finish_slot(slot, mixes, stats):
        absorb(k_first[last, early:], v_first[last, early:], q_slots[slot], slot, False)
        total = run_sum[slot]
        mixes[slot] = (run_out[slot] / total).astype(BF16)
        stats[slot] = jnp.concatenate([run_max[slot], total], axis=0)

    @pl.loop(1, n_sp)
    def _(d):
        finish_slot(sp_at(d), mix_send, stat_send)
        for copy in mix_copies(d, z):
            copy.start()

    with SC("finish_me"):
        finish_slot(z, mix_recv, stat_recv)
        project_pair(last, CHUNKS - 1, tp_at(2 * last), lax.rem(sib + 2 * last, n_tp), (1,))
    with SC("transpose"):
        loads[6].wait()
        loads[7].wait()
        stripe = 2 * HEAD

        @pl.loop(0, width // stripe)
        def _(index):
            place = pl.ds(pl.multiple_of(index * stripe, stripe), stripe)
            w_gate[place, :] = gate_t[:, place].T
            w_value[place, :] = value_t[:, place].T

    with SC("mixwait"):
        for d in range(1, n_sp):
            for copy in mix_copies(d, sp_at(d)):
                copy.wait_recv()
    with SC("kv_a"):
        for block in range(1, n_chip):
            kv_hop(block, 1, arrive=False)
    top = stat_recv[0, 0:1]
    for slot in range(1, n_sp):
        top = jnp.maximum(top, stat_recv[slot, 0:1])
    weight_sum = jnp.zeros_like(top)
    weighted = jnp.zeros(run_out.shape[1:], F32)
    for slot in range(n_sp):
        share = jnp.exp2((stat_recv[slot, 0:1] - top) * EXP_SCALE) * stat_recv[slot, 1:2]
        weight_sum = weight_sum + share
        weighted = weighted + mix_recv[slot].astype(F32) * share
    loads[5].wait()
    with SC("rs0"):
        mixed = scatter_sum(0, head_rows(weighted / weight_sum), out_first)
    after_first = target_v[...].astype(F32) + normed(mixed, post_first[...])
    stream[...] = after_first

    def halo_copy(device):
        return pltpu.make_async_remote_copy(
            src_ref=halo_send, dst_ref=halo_recv, send_sem=halo_sem.at[0],
            recv_sem=halo_sem.at[1], device_id=device, device_id_type=MESH,
        )

    ffn_input = normed(after_first, ffn_pre[...])

    @pl.when(gives_halo)
    def _():
        halo_send[...] = ffn_input[rows - 2 :].astype(BF16)
        for t in range(n_tp):
            halo_copy({"sp": z + 1, "tp": t}).start()

    gather_start(1, ffn_input)
    with SC("kv_b"):
        kv_hop(0, 2)

    def halo_rows():
        @pl.when(z > 0)
        def _():
            halo_copy({"sp": z, "tp": sib}).wait_recv()

        zeros = jnp.zeros((14, width), F32)
        return jnp.concatenate([halo_recv[...].astype(F32), zeros], axis=0).astype(BF16)

    with SC("ag1_up"):
        up_gate, up_value = (
            up.astype(BF16) for up in gather_times(1, [w_gate, w_value], halo_rows)
        )

    def causal_mix(up_rows, taps):
        here = up_rows[:block_rows].astype(F32)
        rim = jnp.where(z > 0, up_rows[block_rows:].astype(F32), 0.0)
        row = lax.broadcasted_iota(jnp.int32, here.shape, 0)
        before = jnp.where(row == 0, rim[1:2], pltpu.roll(here, 1, 0))
        earlier = jnp.where(
            row == 0, rim[0:1], jnp.where(row == 1, rim[1:2], pltpu.roll(here, 2, 0))
        )
        return taps[0:1] * earlier + taps[1:2] * before + taps[2:3] * here

    with SC("gated"):
        gated = (
            jax.nn.gelu(causal_mix(up_gate, conv_gate[...]), approximate=True)
            * causal_mix(up_value, conv_value[...])
        ).astype(BF16)
        loads[8].wait()
    with SC("kv_c"):
        for block in range(1, n_chip):
            kv_hop(block, 2)
    with SC("rs1"):
        ffn_sum = scatter_sum(1, gated, w_down)
    after_ffn = stream[...] + normed(ffn_sum, ffn_post[...])
    stream[...] = after_ffn

    gather_start(2, normed(after_ffn, pre_second[...]))
    with SC("kv_d"):
        for block in range(n_chip):
            kv_hop(block, 3)
    with SC("ag2_q"):
        loads[9].wait()
        queries = head_columns(gather_times(2, [query_second])[0])
        for d in range(1, n_sp):
            q_copy(d, None).wait_send()
        q_slots[z] = queries

    with SC("attn2_own"):
        for block in range(n_chip):
            absorb(k_second[z, block], v_second[z, block], q_slots[z], 0, block == 0)

    with SC("kv_e"):
        @pl.loop(4, max(n_sp, 4) + 1)
        def _(hop):
            for block in range(n_chip):
                kv_hop(block, hop)

    with SC("attn2_rest"):
        @pl.loop(1, n_sp)
        def _(d):
            slot = sp_at(d)
            for block in range(n_chip):
                absorb(k_second[slot, block], v_second[slot, block], q_slots[z], 0, False)

    with SC("rs2"):
        loads[10].wait()
        mixed = scatter_sum(2, head_rows(run_out[0] / run_sum[0]), out_second)
    decoded[...] = stream[...] + normed(mixed, post_second[...])

    for phase in range(3):
        gather_drain(phase)
        sum_drain(phase)
    for c in range(CHUNKS):
        for _ in range(n_chip):
            src_copy(me, c, sib, 0).wait_send()
        for d in range(1, n_chip):
            src_copy(me, c, sib, 1).wait_send()

    def drain(d):
        for block in range(n_chip):
            kv_drain(block, d)
        for copy in mix_copies(d, z):
            copy.wait_send()

    times(1, n_sp, drain)

    @pl.when(gives_halo)
    def _():
        for t in range(n_tp):
            halo_copy({"sp": z, "tp": sib}).wait_send()


def per_device(*arrays):
    (target, source, source_gain, pre_first, query_first, keyval_first, out_first, post_first,
     ffn_pre, w_gate, w_value, conv_gate, conv_value, w_down, ffn_post, pre_second,
     query_second, keyval_second, out_second, post_second) = arrays
    n_tp, n_sp = lax.axis_size("tp"), lax.axis_size("sp")
    sharers = 2 * HEAD // keyval_first.shape[1]
    if sharers > 1:
        groups = [list(range(low, low + sharers)) for low in range(0, n_tp, sharers)]
        keyval_first, keyval_second = (
            lax.all_gather(w, "tp", axis=1, tiled=True, axis_index_groups=groups)
            for w in (keyval_first, keyval_second)
        )
    rows, width = target.shape
    lines = source.shape[0]
    block_rows = rows * n_tp
    columns = query_first.shape[1] // HEAD * block_rows
    n_chip = n_tp // 2
    span = width // PIECES
    dma = pltpu.SemaphoreType.DMA
    any_spec = pl.BlockSpec(memory_space=pl.ANY)
    vmem = pl.BlockSpec(memory_space=pltpu.VMEM)

    def row(gain):
        return gain.reshape(1, width)

    scratch = [
        pltpu.VMEM(target.shape, BF16),
        pltpu.VMEM(source.shape, BF16),
        *(pltpu.VMEM(w.shape, BF16) for w in (
            query_first, keyval_first, out_first, w_gate.T, w_value.T, w_gate, w_value, w_down,
            query_second, keyval_second, out_second)),
        dma((11,)),
        pltpu.VMEM((3, PIECES, n_tp, rows, span), BF16),
        dma((3,)),
        dma((3, PIECES, n_tp)),
        pltpu.VMEM((n_tp, CHUNKS, lines // CHUNKS, width), BF16),
        dma((2,)),
        dma((n_tp, CHUNKS)),
        pltpu.VMEM((n_sp, HEAD, columns), BF16),
        dma((2, n_sp)),
        pltpu.VMEM((n_chip, 2 * lines, HEAD), BF16),
        pltpu.VMEM((n_chip, 2 * lines, HEAD), BF16),
        pltpu.VMEM((n_sp, n_chip, 2 * lines, HEAD), BF16),
        pltpu.VMEM((n_sp, n_chip, 2 * lines, HEAD), BF16),
        dma((2,)),
        dma((2, n_sp, n_chip)),
        pltpu.VMEM((n_sp, 1, columns), F32),
        pltpu.VMEM((n_sp, 1, columns), F32),
        pltpu.VMEM((n_sp, HEAD, columns), F32),
        pltpu.VMEM((n_sp, HEAD, columns), BF16),
        pltpu.VMEM((n_sp, HEAD, columns), BF16),
        pltpu.VMEM((n_sp, 2, columns), F32),
        pltpu.VMEM((n_sp, 2, columns), F32),
        dma((2, 2, n_sp)),
        pltpu.VMEM((3, PIECES, 2, n_chip, rows, span), BF16),
        pltpu.VMEM((3, PIECES, n_chip, rows, span), BF16),
        pltpu.VMEM((3, PIECES, n_chip, rows, span), BF16),
        pltpu.VMEM((3, PIECES, n_chip, rows, span), BF16),
        dma((3, 2)),
        dma((3, PIECES)),
        dma((3, PIECES, n_chip)),
        pltpu.VMEM((2, width), BF16),
        pltpu.VMEM((2, width), BF16),
        dma((2,)),
        pltpu.VMEM((rows, width), F32),
    ]

    def kernel(*refs):
        decoder_kernel(n_tp, n_sp, *refs)

    return pl.pallas_call(
        kernel,
        out_shape=jax.ShapeDtypeStruct((rows, width), F32),
        in_specs=[any_spec, any_spec, vmem, vmem, any_spec, any_spec, any_spec, vmem, vmem,
                  any_spec, any_spec, vmem, vmem, any_spec, vmem, vmem, any_spec, any_spec,
                  any_spec, vmem],
        out_specs=vmem,
        scratch_shapes=scratch,
        compiler_params=pltpu.CompilerParams(
            collective_id=0, has_side_effects=True, vmem_limit_bytes=67_000_000
        ),
        name="decoder",
    )(
        target, source, row(source_gain), row(pre_first), query_first, keyval_first, out_first,
        row(post_first), row(ffn_pre), w_gate.T, w_value.T, conv_gate, conv_value, w_down,
        row(ffn_post), row(pre_second), query_second, keyval_second, out_second, row(post_second),
    )


def solution(mesh):
    rows = P(("grp", "sp", "tp"), None)
    by_column, by_row = P(None, "tp"), P("tp", None)
    placed = (
        rows, rows, P(), P(), by_column, by_column, by_row, P(), P(), by_column, by_column,
        by_column, by_column, by_row, P(), P(), by_column, by_column, by_row, P(),
    )
    return jax.shard_map(
        per_device, mesh=mesh, in_specs=placed, out_specs=rows, check_vma=False
    )
```

```python
import math

import jax
import jax.numpy as jnp
from jax import lax
from jax.experimental import pallas as pl
from jax.experimental.pallas import tpu as pltpu
from jax.sharding import PartitionSpec as P

HEAD = 128
CHUNKS = 4
PIECES = 2
EXP_SCALE = HEAD ** (-0.5) * math.log2(math.e)
F32, BF16 = jnp.float32, jnp.bfloat16
MESH = pl.DeviceIdType.MESH


def normed(values, gain):
    widened = values.astype(F32)
    return widened * lax.rsqrt(jnp.mean(widened * widened, axis=-1, keepdims=True) + 1e-06) * gain


SC = jax.named_scope


def times(start, stop, body):
    if stop - start <= 4:
        for index in range(start, stop):
            body(index)
    else:

        @pl.loop(start, stop)
        def _(index):
            body(index)


def dot(left, right):
    return jnp.dot(left, right, preferred_element_type=F32)


def decoder_kernel(
    n_tp,
    n_sp,
    target_h,
    source_h,
    source_gain_h,
    pre_first_h,
    query_first_h,
    keyval_first_h,
    out_first_h,
    post_first_h,
    ffn_pre_h,
    gate_h,
    value_h,
    conv_gate_h,
    conv_value_h,
    down_h,
    ffn_post_h,
    pre_second_h,
    query_second_h,
    keyval_second_h,
    out_second_h,
    post_second_h,
    decoded,
    source_gain,
    pre_first,
    post_first,
    ffn_pre,
    conv_gate,
    conv_value,
    ffn_post,
    pre_second,
    post_second,
    vec_sem,
    target_v,
    source_v,
    query_first,
    keyval_first,
    out_first,
    gate_t,
    value_t,
    w_gate,
    w_value,
    w_down,
    query_second,
    keyval_second,
    out_second,
    local_sem,
    hidden,
    hidden_send,
    hidden_recv,
    src,
    src_send,
    src_recv,
    q_slots,
    q_sem,
    k_first,
    v_first,
    kv_second,
    kv_send,
    kv_recv,
    run_max,
    run_sum,
    run_out,
    mix_send,
    mix_recv,
    stat_send,
    stat_recv,
    mix_sem,
    part,
    pair_recv,
    pair_sum,
    part_recv,
    part_send,
    pair_sem,
    part_sem,
    halo_send,
    halo_recv,
    halo_sem,
    stream,
):
    me = lax.axis_index("tp")
    z = lax.axis_index("sp")
    sib = me + 1 - 2 * lax.rem(me, 2)
    core, chip = lax.rem(me, 2), me // 2
    n_chip = n_tp // 2
    rows = target_v.shape[0]
    width = target_v.shape[1]
    span = width // PIECES
    chunk = src.shape[2]
    block_rows = rows * n_tp

    def tp_at(distance):
        return lax.rem(me + distance, n_tp)

    def sp_at(distance):
        return lax.rem(z + distance, n_sp)

    def to_tp(source, dest, send, recv, device):
        return pltpu.make_async_remote_copy(
            src_ref=source, dst_ref=dest, send_sem=send, recv_sem=recv,
            device_id={"tp": device}, device_id_type=MESH,
        )

    def to_sp(source, dest, send, recv, device):
        return pltpu.make_async_remote_copy(
            src_ref=source, dst_ref=dest, send_sem=send, recv_sem=recv,
            device_id={"sp": device}, device_id_type=MESH,
        )

    pairs = [
        (target_h, target_v),
        (source_h, source_v),
        (query_first_h, query_first),
        (keyval_first_h, keyval_first),
        (keyval_second_h, keyval_second),
        (out_first_h, out_first),
        (gate_h, gate_t),
        (value_h, value_t),
        (down_h, w_down),
        (query_second_h, query_second),
        (out_second_h, out_second),
    ]
    loads = [
        pltpu.make_async_copy(a, b, local_sem.at[i]) for i, (a, b) in enumerate(pairs)
    ]
    vectors = {
        name: pltpu.make_async_copy(a, b, vec_sem.at[i])
        for i, (name, a, b) in enumerate([
            ("pre_first", pre_first_h, pre_first),
            ("source_gain", source_gain_h, source_gain),
            ("post_first", post_first_h, post_first),
            ("ffn_pre", ffn_pre_h, ffn_pre),
            ("conv_gate", conv_gate_h, conv_gate),
            ("conv_value", conv_value_h, conv_value),
            ("ffn_post", ffn_post_h, ffn_post),
            ("pre_second", pre_second_h, pre_second),
            ("post_second", post_second_h, post_second),
        ])
    }
    loads[0].start()
    vectors["pre_first"].start()
    vectors["source_gain"].start()
    for load in loads[1:]:
        load.start()
    for name in list(vectors)[2:]:
        vectors[name].start()

    barrier = pltpu.get_barrier_semaphore()
    for distance in range(1, n_tp):
        pl.semaphore_signal(barrier, inc=1, device_id={"tp": tp_at(distance)}, device_id_type=MESH)
    for distance in range(1, n_sp):
        pl.semaphore_signal(barrier, inc=1, device_id={"sp": sp_at(distance)}, device_id_type=MESH)
    last_tp = n_tp - 1

    @pl.when(jnp.logical_and(z > 0, me < last_tp))
    def _():
        pl.semaphore_signal(
            barrier, inc=1, device_id={"sp": z - 1, "tp": last_tp}, device_id_type=MESH
        )

    gives_halo = jnp.logical_and(me == last_tp, z < n_sp - 1)
    with SC("barrier"):
        pl.semaphore_wait(barrier, n_tp - 1 + n_sp - 1 + jnp.where(gives_halo, n_tp - 1, 0))

    def hidden_copy(phase, piece, slot, device):
        return to_tp(
            hidden.at[phase, piece, slot], hidden.at[phase, piece, slot],
            hidden_send.at[phase], hidden_recv.at[phase, piece, slot], device,
        )

    def gather_start(phase, value):
        for piece in range(PIECES):
            hidden[phase, piece, me] = value[:, piece * span : (piece + 1) * span].astype(BF16)
            for d in range(1, n_chip):
                hidden_copy(phase, piece, me, tp_at(2 * d)).start()
            hidden_copy(phase, piece, me, sib).start()

    def gather_times(phase, weights, extra=None):
        totals = [None] * len(weights)
        for piece in range(PIECES + 1):
            if piece < PIECES:
                for d in range(1, n_chip):
                    slot = tp_at(2 * d)
                    hidden_copy(phase, piece, slot, sib).wait_recv()
                    hidden_copy(phase, piece, slot, sib).start()
            if piece == 0:
                continue
            ready = piece - 1
            for d in range(n_chip):
                slot = lax.rem(sib + 2 * d, n_tp)
                hidden_copy(phase, ready, slot, sib).wait_recv()
            whole = hidden[phase, ready]
            if rows % 16:
                whole = whole.astype(F32).reshape(block_rows, span).astype(BF16)
            else:
                whole = whole.reshape(block_rows, span)
            if extra is not None:
                if ready == 0:
                    rim = extra()
                whole = jnp.concatenate([whole, rim[:, ready * span : (ready + 1) * span]], axis=0)
            for index, weight in enumerate(weights):
                product = dot(whole, weight[ready * span : (ready + 1) * span, :])
                totals[index] = product if ready == 0 else totals[index] + product
        return totals

    def gather_drain(phase):
        for piece in range(PIECES):
            for _ in range(2 * n_chip - 1):
                hidden_copy(phase, piece, me, sib).wait_send()

    def pair_copy(phase, piece):
        return to_tp(
            part.at[phase, piece, 1 - core], pair_recv.at[phase, piece],
            part_send.at[phase, 0], pair_sem.at[phase, piece], sib,
        )

    def chip_copy(phase, piece, distance, slot):
        other = lax.rem(chip + distance, n_chip)
        return to_tp(
            pair_sum.at[phase, piece, other], part_recv.at[phase, piece, slot],
            part_send.at[phase, 1], part_sem.at[phase, piece, slot], 2 * other + core,
        )

    def scatter_sum(phase, left, weight):
        for piece in range(PIECES):
            product = dot(left, weight[:, piece * span : (piece + 1) * span])
            product = product.reshape(n_chip, 2, rows, span)
            for parity in range(2):
                part[phase, piece, parity] = product[:, parity].astype(BF16)
            pair_copy(phase, piece).start()
        for piece in range(PIECES):
            pair_copy(phase, piece).wait_recv()
            mine = part[phase, piece, core].astype(F32)
            pair_sum[phase, piece] = (mine + pair_recv[phase, piece].astype(F32)).astype(BF16)
            for d in range(1, n_chip):
                chip_copy(phase, piece, d, chip).start()
        sums = []
        for piece in range(PIECES):
            total = pair_sum[phase, piece, chip].astype(F32)
            for d in range(1, n_chip):
                slot = lax.rem(chip + d, n_chip)
                chip_copy(phase, piece, d, slot).wait_recv()
                total = total + part_recv[phase, piece, slot].astype(F32)
            sums.append(total)
        return jnp.concatenate(sums, axis=1)

    def sum_drain(phase):
        for piece in range(PIECES):
            pair_copy(phase, piece).wait_send()
            for d in range(1, n_chip):
                chip_copy(phase, piece, d, chip).wait_send()

    def head_columns(queries):
        blocks = [
            queries[:, h : h + HEAD].T for h in range(0, queries.shape[1], HEAD)
        ]
        return jnp.concatenate(blocks, axis=1).astype(BF16)

    def head_rows(columns):
        blocks = [
            columns[:, c : c + block_rows].T for c in range(0, columns.shape[1], block_rows)
        ]
        return jnp.concatenate(blocks, axis=1).astype(BF16)

    loads[0].wait()
    vectors["pre_first"].wait()
    with SC("norm0"):
        gather_start(0, normed(target_v[...], pre_first[...]))

    def src_copy(slot, c, device, kind):
        return to_tp(
            src.at[slot, c], src.at[slot, c], src_send.at[kind], src_recv.at[slot, c], device
        )

    loads[1].wait()
    vectors["source_gain"].wait()
    for c in range(CHUNKS):
        src[me, c] = normed(source_v[pl.ds(c * chunk, chunk)], source_gain[...]).astype(BF16)
        for d in range(1, n_chip):
            src_copy(me, c, tp_at(2 * d), 0).start()
        src_copy(me, c, sib, 0).start()

    loads[2].wait()
    with SC("qproj"):
        q_slots[z] = head_columns(gather_times(0, [query_first])[0])

    def q_copy(distance, slot):
        return to_sp(
            q_slots.at[z], q_slots.at[z] if slot is None else q_slots.at[slot],
            q_sem.at[0, 0], q_sem.at[1, z if slot is None else slot], sp_at(distance),
        )

    for d in range(1, n_sp):
        q_copy(d, None).start()

    loads[3].wait()
    loads[4].wait()

    def project_pair(block, c, mine, other, layers=(0, 1)):
        lines = jnp.concatenate([src[mine, c], src[other, c]], axis=0)
        place = pl.ds(c * 2 * chunk, 2 * chunk)
        if 0 in layers:
            first = dot(lines, keyval_first[...])
            k_first[block, place] = first[:, :HEAD].astype(BF16)
            v_first[block, place] = first[:, HEAD:].astype(BF16)
        if 1 in layers:
            second = dot(lines, keyval_second[...])
            kv_second[z, block, c, 0] = second[:, :HEAD].astype(BF16)
            kv_second[z, block, c, 1] = second[:, HEAD:].astype(BF16)

    def absorb(keys, values, queries, slot, fresh):
        scores = dot(keys, queries)
        newest = jnp.max(scores, axis=0, keepdims=True)
        if not fresh:
            newest = jnp.maximum(newest, run_max[slot])
        weights = jnp.exp2((scores - newest) * EXP_SCALE)
        added = jnp.sum(weights, axis=0, keepdims=True)
        gathered = lax.dot_general(
            values, weights.astype(BF16), (((0,), (0,)), ((), ())), preferred_element_type=F32
        )
        if not fresh:
            rescale = jnp.exp2((run_max[slot] - newest) * EXP_SCALE)
            added = added + run_sum[slot] * rescale
            gathered = gathered + run_out[slot] * rescale
        run_max[slot] = newest
        run_sum[slot] = added
        run_out[slot] = gathered

    def absorb_block(block, fresh):
        @pl.loop(0, n_sp)
        def _(slot):
            absorb(k_first[block], v_first[block], q_slots[slot], slot, fresh)

    def kv_copy(block, slot, c, peer):
        held = kv_second.at[slot, block, c]
        return to_sp(held, held, kv_send, kv_recv.at[slot, block, c], peer)

    def kv_hop(block, hop, arrive=True, chunks=range(CHUNKS)):
        for step in (1, -1):
            slot = z - step * (hop - 1)
            peer = z + step

            @pl.when(jnp.logical_and(slot >= 0, slot < n_sp))
            def _():
                if arrive:
                    for c in chunks:
                        kv_copy(block, slot, c, sp_at(1)).wait_recv()

                @pl.when(jnp.logical_and(hop < n_sp, jnp.logical_and(peer >= 0, peer < n_sp)))
                def _():
                    for c in chunks:
                        kv_copy(block, slot, c, peer).start()

    def kv_drain(block, hop):
        for step in (1, -1):
            slot = z - step * (hop - 1)
            peer = z + step
            inside = jnp.logical_and(slot >= 0, slot < n_sp)

            @pl.when(jnp.logical_and(inside, jnp.logical_and(peer >= 0, peer < n_sp)))
            def _():
                for c in range(CHUNKS):
                    kv_copy(block, slot, c, peer).wait_send()

    def nearest(j):
        up = j + jnp.where(j >= z, 1, 0)
        down = n_sp - 1 - j
        down = down - jnp.where(down <= z, 1, 0)
        return jnp.where(2 * z < n_sp, up, down)

    def second_rows(slot, part):
        return kv_second[slot, :, :, part].reshape(n_chip * CHUNKS * 2 * chunk, HEAD)

    for c in range(CHUNKS):
        src_copy(sib, c, sib, 0).wait_recv()
        project_pair(0, c, me, sib)
    for d in range(1, n_sp):
        q_copy(d, sp_at(d)).wait_recv()
    kv_hop(0, 1, arrive=False)
    with SC("abs_own"):
        absorb_block(0, True)

    def far_chunk(d, c, layers=(0, 1)):
        near = tp_at(2 * d)
        far = lax.rem(sib + 2 * d, n_tp)
        src_copy(near, c, sib, 1).wait_recv()
        src_copy(near, c, sib, 1).start()
        src_copy(far, c, sib, 1).wait_recv()
        project_pair(d, c, near, far, layers)

    def far_absorb(d):
        for c in range(CHUNKS):
            far_chunk(d, c)
        absorb_block(d, False)

    times(1, n_chip - 1, far_absorb)
    last = n_chip - 1
    early = (CHUNKS - 1) * 2 * chunk
    with SC("far_early"):
        for c in range(CHUNKS - 1):
            far_chunk(last, c)
            if n_chip > 1:
                kv_hop(last, 1, False, (c,))

    with SC("abs_early"):
        @pl.loop(0, n_sp)
        def _(slot):
            absorb(k_first[last, :early], v_first[last, :early], q_slots[slot], slot, False)

    with SC("far_last"):
        far_chunk(last, CHUNKS - 1, (0,))

    def mix_copies(peer, slot):
        return [
            to_sp(sent.at[peer], got.at[slot], mix_sem.at[index, 0, 0], mix_sem.at[index, 1, slot], peer)
            for index, (sent, got) in enumerate(((mix_send, mix_recv), (stat_send, stat_recv)))
        ]

    def finish_slot(slot, mixes, stats):
        absorb(k_first[last, early:], v_first[last, early:], q_slots[slot], slot, False)
        total = run_sum[slot]
        mixes[slot] = (run_out[slot] / total).astype(BF16)
        stats[slot] = jnp.concatenate([run_max[slot], total], axis=0)

    @pl.loop(0, n_sp - 1)
    def _(j):
        peer = nearest(n_sp - 2 - j)
        finish_slot(peer, mix_send, stat_send)
        for copy in mix_copies(peer, z):
            copy.start()

    with SC("finish_me"):
        finish_slot(z, mix_recv, stat_recv)
        project_pair(last, CHUNKS - 1, tp_at(2 * last), lax.rem(sib + 2 * last, n_tp), (1,))
    with SC("transpose"):
        loads[6].wait()
        loads[7].wait()
        for name in list(vectors)[2:]:
            vectors[name].wait()
        stripe = 2 * HEAD

        @pl.loop(0, width // stripe)
        def _(index):
            place = pl.ds(pl.multiple_of(index * stripe, stripe), stripe)
            w_gate[place, :] = gate_t[:, place].T
            w_value[place, :] = value_t[:, place].T

    with SC("mixwait"):
        for d in range(1, n_sp):
            for copy in mix_copies(sp_at(d), sp_at(d)):
                copy.wait_recv()
    with SC("kv_a"):
        kv_hop(last, 1, False, (CHUNKS - 1,))
        for block in range(1, last):
            kv_hop(block, 1, False)
        kv_hop(0, 2)
    top = stat_recv[0, 0:1]
    for slot in range(1, n_sp):
        top = jnp.maximum(top, stat_recv[slot, 0:1])
    weight_sum = jnp.zeros_like(top)
    weighted = jnp.zeros(run_out.shape[1:], F32)
    for slot in range(n_sp):
        share = jnp.exp2((stat_recv[slot, 0:1] - top) * EXP_SCALE) * stat_recv[slot, 1:2]
        weight_sum = weight_sum + share
        weighted = weighted + mix_recv[slot].astype(F32) * share
    loads[5].wait()
    with SC("rs0"):
        mixed = scatter_sum(0, head_rows(weighted / weight_sum), out_first)
    after_first = target_v[...].astype(F32) + normed(mixed, post_first[...])
    stream[...] = after_first

    def halo_copy(device):
        return pltpu.make_async_remote_copy(
            src_ref=halo_send, dst_ref=halo_recv, send_sem=halo_sem.at[0],
            recv_sem=halo_sem.at[1], device_id=device, device_id_type=MESH,
        )

    ffn_input = normed(after_first, ffn_pre[...])

    @pl.when(gives_halo)
    def _():
        halo_send[...] = ffn_input[rows - 2 :].astype(BF16)
        for t in range(n_tp):
            halo_copy({"sp": z + 1, "tp": t}).start()

    gather_start(1, ffn_input)
    with SC("kv_b"):
        for block in range(1, n_chip):
            kv_hop(block, 2)

    def halo_rows():
        @pl.when(z > 0)
        def _():
            halo_copy({"sp": z, "tp": sib}).wait_recv()

        zeros = jnp.zeros((14, width), F32)
        return jnp.concatenate([halo_recv[...].astype(F32), zeros], axis=0).astype(BF16)

    with SC("ag1_up"):
        up_gate, up_value = (
            up.astype(BF16) for up in gather_times(1, [w_gate, w_value], halo_rows)
        )

    def causal_mix(up_rows, taps):
        here = up_rows[:block_rows].astype(F32)
        rim = jnp.where(z > 0, up_rows[block_rows:].astype(F32), 0.0)
        row = lax.broadcasted_iota(jnp.int32, here.shape, 0)
        before = jnp.where(row == 0, rim[1:2], pltpu.roll(here, 1, 0))
        earlier = jnp.where(
            row == 0, rim[0:1], jnp.where(row == 1, rim[1:2], pltpu.roll(here, 2, 0))
        )
        return taps[0:1] * earlier + taps[1:2] * before + taps[2:3] * here

    with SC("gated"):
        gated = (
            jax.nn.gelu(causal_mix(up_gate, conv_gate[...]), approximate=True)
            * causal_mix(up_value, conv_value[...])
        ).astype(BF16)
        loads[8].wait()
    with SC("kv_c"):
        kv_hop(0, 3)
    with SC("rs1"):
        ffn_sum = scatter_sum(1, gated, w_down)
    after_ffn = stream[...] + normed(ffn_sum, ffn_post[...])
    stream[...] = after_ffn

    gather_start(2, normed(after_ffn, pre_second[...]))
    with SC("kv_d"):
        for block in range(1, n_chip):
            kv_hop(block, 3)
    with SC("ag2_q"):
        loads[9].wait()
        queries = head_columns(gather_times(2, [query_second])[0])
        for d in range(1, n_sp):
            q_copy(d, None).wait_send()
        q_slots[z] = queries

    with SC("attn2_own"):
        absorb(second_rows(z, 0), second_rows(z, 1), q_slots[z], 0, True)

    def kv_rest():
        @pl.loop(4, max(n_sp, 4) + 1)
        def _(hop):
            for block in range(n_chip):
                kv_hop(block, hop)

    def absorb_second(j):
        slot = nearest(j)
        absorb(second_rows(slot, 0), second_rows(slot, 1), q_slots[z], 0, False)

    with SC("attn2_rest"):
        if n_sp > 4:
            kv_rest()
        times(0, n_sp - 2, absorb_second)
    with SC("kv_e"):
        if n_sp <= 4:
            kv_rest()
    with SC("attn2_last"):
        absorb_second(n_sp - 2)

    with SC("rs2"):
        loads[10].wait()
        mixed = scatter_sum(2, head_rows(run_out[0] / run_sum[0]), out_second)
    decoded[...] = stream[...] + normed(mixed, post_second[...])

    for phase in range(3):
        gather_drain(phase)
        sum_drain(phase)
    for c in range(CHUNKS):
        for _ in range(n_chip):
            src_copy(me, c, sib, 0).wait_send()
        for d in range(1, n_chip):
            src_copy(me, c, sib, 1).wait_send()

    def drain(d):
        for block in range(n_chip):
            kv_drain(block, d)
        for copy in mix_copies(sp_at(d), z):
            copy.wait_send()

    times(1, n_sp, drain)

    @pl.when(gives_halo)
    def _():
        for t in range(n_tp):
            halo_copy({"sp": z, "tp": sib}).wait_send()


def per_device(*arrays):
    (target, source, source_gain, pre_first, query_first, keyval_first, out_first, post_first,
     ffn_pre, w_gate, w_value, conv_gate, conv_value, w_down, ffn_post, pre_second,
     query_second, keyval_second, out_second, post_second) = arrays
    n_tp, n_sp = lax.axis_size("tp"), lax.axis_size("sp")
    sharers = 2 * HEAD // keyval_first.shape[1]
    if sharers > 1:
        groups = [list(range(low, low + sharers)) for low in range(0, n_tp, sharers)]
        keyval_first, keyval_second = (
            lax.all_gather(w, "tp", axis=1, tiled=True, axis_index_groups=groups)
            for w in (keyval_first, keyval_second)
        )
    rows, width = target.shape
    lines = source.shape[0]
    block_rows = rows * n_tp
    columns = query_first.shape[1] // HEAD * block_rows
    n_chip = n_tp // 2
    span = width // PIECES
    dma = pltpu.SemaphoreType.DMA
    hbm = pl.BlockSpec(memory_space=pltpu.HBM)
    vmem = pl.BlockSpec(memory_space=pltpu.VMEM)

    def row(gain):
        return gain.reshape(1, width)

    line = pltpu.VMEM((1, width), F32)
    scratch = [
        *([line] * 4), pltpu.VMEM(conv_gate.shape, F32), pltpu.VMEM(conv_value.shape, F32),
        *([line] * 3), dma((9,)),
        pltpu.VMEM(target.shape, BF16),
        pltpu.VMEM(source.shape, BF16),
        *(pltpu.VMEM(w.shape, BF16) for w in (
            query_first, keyval_first, out_first, w_gate.T, w_value.T, w_gate, w_value, w_down,
            query_second, keyval_second, out_second)),
        dma((11,)),
        pltpu.VMEM((3, PIECES, n_tp, rows, span), BF16),
        dma((3,)),
        dma((3, PIECES, n_tp)),
        pltpu.VMEM((n_tp, CHUNKS, lines // CHUNKS, width), BF16),
        dma((2,)),
        dma((n_tp, CHUNKS)),
        pltpu.VMEM((n_sp, HEAD, columns), BF16),
        dma((2, n_sp)),
        pltpu.VMEM((n_chip, 2 * lines, HEAD), BF16),
        pltpu.VMEM((n_chip, 2 * lines, HEAD), BF16),
        pltpu.VMEM((n_sp, n_chip, CHUNKS, 2, 2 * lines // CHUNKS, HEAD), BF16),
        dma,
        dma((n_sp, n_chip, CHUNKS)),
        pltpu.VMEM((n_sp, 1, columns), F32),
        pltpu.VMEM((n_sp, 1, columns), F32),
        pltpu.VMEM((n_sp, HEAD, columns), F32),
        pltpu.VMEM((n_sp, HEAD, columns), BF16),
        pltpu.VMEM((n_sp, HEAD, columns), BF16),
        pltpu.VMEM((n_sp, 2, columns), F32),
        pltpu.VMEM((n_sp, 2, columns), F32),
        dma((2, 2, n_sp)),
        pltpu.VMEM((3, PIECES, 2, n_chip, rows, span), BF16),
        pltpu.VMEM((3, PIECES, n_chip, rows, span), BF16),
        pltpu.VMEM((3, PIECES, n_chip, rows, span), BF16),
        pltpu.VMEM((3, PIECES, n_chip, rows, span), BF16),
        dma((3, 2)),
        dma((3, PIECES)),
        dma((3, PIECES, n_chip)),
        pltpu.VMEM((2, width), BF16),
        pltpu.VMEM((2, width), BF16),
        dma((2,)),
        pltpu.VMEM((rows, width), F32),
    ]

    def kernel(*refs):
        decoder_kernel(n_tp, n_sp, *refs)

    return pl.pallas_call(
        kernel,
        out_shape=pltpu.VMEM((rows, width), F32),
        in_specs=[hbm] * 20,
        out_specs=vmem,
        scratch_shapes=scratch,
        compiler_params=pltpu.CompilerParams(
            collective_id=0, has_side_effects=True, vmem_limit_bytes=60_000_000
        ),
        name="decoder",
    )(
        target, source, row(source_gain), row(pre_first), query_first, keyval_first, out_first,
        row(post_first), row(ffn_pre), w_gate.T, w_value.T, conv_gate, conv_value, w_down,
        row(ffn_post), row(pre_second), query_second, keyval_second, out_second, row(post_second),
    )


def solution(mesh):
    rows = P(("grp", "sp", "tp"), None)
    by_column, by_row = P(None, "tp"), P("tp", None)
    placed = (
        rows, rows, P(), P(), by_column, by_column, by_row, P(), P(), by_column, by_column,
        by_column, by_column, by_row, P(), P(), by_column, by_column, by_row, P(),
    )
    return jax.shard_map(
        per_device, mesh=mesh, in_specs=placed, out_specs=rows, check_vma=False
    )
```

```python
import math

import jax
import jax.numpy as jnp
from jax import lax
from jax.experimental import pallas as pl
from jax.experimental.pallas import tpu as pltpu
from jax.sharding import PartitionSpec as P

HEAD = 128
CHUNKS = 4
PIECES = 2
EXP_SCALE = HEAD ** (-0.5) * math.log2(math.e)
F32, BF16 = jnp.float32, jnp.bfloat16
MESH = pl.DeviceIdType.MESH


def normed(values, gain):
    widened = values.astype(F32)
    return widened * lax.rsqrt(jnp.mean(widened * widened, axis=-1, keepdims=True) + 1e-06) * gain


SC = jax.named_scope


def times(start, stop, body):
    if stop - start <= 4:
        for index in range(start, stop):
            body(index)
    else:

        @pl.loop(start, stop)
        def _(index):
            body(index)


def dot(left, right):
    return jnp.dot(left, right, preferred_element_type=F32)


def decoder_kernel(
    n_tp,
    n_sp,
    target_h,
    source_h,
    source_gain_h,
    pre_first_h,
    query_first_h,
    keyval_first_h,
    out_first_h,
    post_first_h,
    ffn_pre_h,
    gate_h,
    value_h,
    conv_gate_h,
    conv_value_h,
    down_h,
    ffn_post_h,
    pre_second_h,
    query_second_h,
    keyval_second_h,
    out_second_h,
    post_second_h,
    decoded,
    source_gain,
    pre_first,
    post_first,
    ffn_pre,
    conv_gate,
    conv_value,
    ffn_post,
    pre_second,
    post_second,
    vec_sem,
    target_v,
    source_v,
    query_first,
    keyval_first,
    out_first,
    gate_t,
    value_t,
    w_gate,
    w_value,
    w_down,
    query_second,
    keyval_second,
    out_second,
    local_sem,
    hidden,
    hidden_send,
    hidden_recv,
    src,
    src_send,
    src_recv,
    q_slots,
    q_sem,
    k_first,
    v_first,
    kv_second,
    kv_send,
    kv_recv,
    run_max,
    run_sum,
    run_out,
    mix_send,
    mix_recv,
    stat_send,
    stat_recv,
    mix_sem,
    part,
    pair_recv,
    pair_sum,
    part_recv,
    part_send,
    pair_sem,
    part_sem,
    halo_send,
    halo_recv,
    halo_sem,
    stream,
    relay_mix,
    relay_stat,
    relay_sem,
):
    me = lax.axis_index("tp")
    z = lax.axis_index("sp")
    sib = me + 1 - 2 * lax.rem(me, 2)
    core, chip = lax.rem(me, 2), me // 2
    n_chip = n_tp // 2
    rows = target_v.shape[0]
    width = target_v.shape[1]
    span = width // PIECES
    chunk = src.shape[2]
    block_rows = rows * n_tp

    def tp_at(distance):
        return lax.rem(me + distance, n_tp)

    def sp_at(distance):
        return lax.rem(z + distance, n_sp)

    def to_tp(source, dest, send, recv, device):
        return pltpu.make_async_remote_copy(
            src_ref=source, dst_ref=dest, send_sem=send, recv_sem=recv,
            device_id={"tp": device}, device_id_type=MESH,
        )

    def to_sp(source, dest, send, recv, device):
        return pltpu.make_async_remote_copy(
            src_ref=source, dst_ref=dest, send_sem=send, recv_sem=recv,
            device_id={"sp": device}, device_id_type=MESH,
        )

    pairs = [
        (target_h, target_v),
        (source_h, source_v),
        (query_first_h, query_first),
        (keyval_first_h, keyval_first),
        (keyval_second_h, keyval_second),
        (out_first_h, out_first),
        (gate_h, gate_t),
        (value_h, value_t),
        (down_h, w_down),
        (query_second_h, query_second),
        (out_second_h, out_second),
    ]
    loads = [
        pltpu.make_async_copy(a, b, local_sem.at[i]) for i, (a, b) in enumerate(pairs)
    ]
    vectors = {
        name: pltpu.make_async_copy(a, b, vec_sem.at[i])
        for i, (name, a, b) in enumerate([
            ("pre_first", pre_first_h, pre_first),
            ("source_gain", source_gain_h, source_gain),
            ("post_first", post_first_h, post_first),
            ("ffn_pre", ffn_pre_h, ffn_pre),
            ("conv_gate", conv_gate_h, conv_gate),
            ("conv_value", conv_value_h, conv_value),
            ("ffn_post", ffn_post_h, ffn_post),
            ("pre_second", pre_second_h, pre_second),
            ("post_second", post_second_h, post_second),
        ])
    }
    loads[0].start()
    vectors["pre_first"].start()
    vectors["source_gain"].start()
    for load in loads[1:]:
        load.start()
    for name in list(vectors)[2:]:
        vectors[name].start()

    barrier = pltpu.get_barrier_semaphore()
    for distance in range(1, n_tp):
        pl.semaphore_signal(barrier, inc=1, device_id={"tp": tp_at(distance)}, device_id_type=MESH)
    for distance in range(1, n_sp):
        pl.semaphore_signal(barrier, inc=1, device_id={"sp": sp_at(distance)}, device_id_type=MESH)
    last_tp = n_tp - 1

    @pl.when(jnp.logical_and(z > 0, me < last_tp))
    def _():
        pl.semaphore_signal(
            barrier, inc=1, device_id={"sp": z - 1, "tp": last_tp}, device_id_type=MESH
        )

    gives_halo = jnp.logical_and(me == last_tp, z < n_sp - 1)
    with SC("barrier"):
        pl.semaphore_wait(barrier, n_tp - 1 + n_sp - 1 + jnp.where(gives_halo, n_tp - 1, 0))

    def hidden_copy(phase, piece, slot, device):
        return to_tp(
            hidden.at[phase, piece, slot], hidden.at[phase, piece, slot],
            hidden_send.at[phase], hidden_recv.at[phase, piece, slot], device,
        )

    def gather_start(phase, value):
        for piece in range(PIECES):
            hidden[phase, piece, me] = value[:, piece * span : (piece + 1) * span].astype(BF16)
            for d in range(1, n_chip):
                hidden_copy(phase, piece, me, tp_at(2 * d)).start()
            hidden_copy(phase, piece, me, sib).start()

    def gather_times(phase, weights, extra=None):
        totals = [None] * len(weights)
        for piece in range(PIECES + 1):
            if piece < PIECES:
                for d in range(1, n_chip):
                    slot = tp_at(2 * d)
                    hidden_copy(phase, piece, slot, sib).wait_recv()
                    hidden_copy(phase, piece, slot, sib).start()
            if piece == 0:
                continue
            ready = piece - 1
            for d in range(n_chip):
                slot = lax.rem(sib + 2 * d, n_tp)
                hidden_copy(phase, ready, slot, sib).wait_recv()
            whole = hidden[phase, ready]
            if rows % 16:
                whole = whole.astype(F32).reshape(block_rows, span).astype(BF16)
            else:
                whole = whole.reshape(block_rows, span)
            if extra is not None:
                if ready == 0:
                    rim = extra()
                whole = jnp.concatenate([whole, rim[:, ready * span : (ready + 1) * span]], axis=0)
            for index, weight in enumerate(weights):
                product = dot(whole, weight[ready * span : (ready + 1) * span, :])
                totals[index] = product if ready == 0 else totals[index] + product
        return totals

    def gather_drain(phase):
        for piece in range(PIECES):
            for _ in range(2 * n_chip - 1):
                hidden_copy(phase, piece, me, sib).wait_send()

    def pair_copy(phase, piece):
        return to_tp(
            part.at[phase, piece, 1 - core], pair_recv.at[phase, piece],
            part_send.at[phase, 0], pair_sem.at[phase, piece], sib,
        )

    def chip_copy(phase, piece, distance, slot):
        other = lax.rem(chip + distance, n_chip)
        return to_tp(
            pair_sum.at[phase, piece, other], part_recv.at[phase, piece, slot],
            part_send.at[phase, 1], part_sem.at[phase, piece, slot], 2 * other + core,
        )

    def scatter_sum(phase, left, weight):
        for piece in range(PIECES):
            product = dot(left, weight[:, piece * span : (piece + 1) * span])
            product = product.reshape(n_chip, 2, rows, span)
            for parity in range(2):
                part[phase, piece, parity] = product[:, parity].astype(BF16)
            pair_copy(phase, piece).start()
        for piece in range(PIECES):
            pair_copy(phase, piece).wait_recv()
            mine = part[phase, piece, core].astype(F32)
            pair_sum[phase, piece] = (mine + pair_recv[phase, piece].astype(F32)).astype(BF16)
            for d in range(1, n_chip):
                chip_copy(phase, piece, d, chip).start()
        sums = []
        for piece in range(PIECES):
            total = pair_sum[phase, piece, chip].astype(F32)
            for d in range(1, n_chip):
                slot = lax.rem(chip + d, n_chip)
                chip_copy(phase, piece, d, slot).wait_recv()
                total = total + part_recv[phase, piece, slot].astype(F32)
            sums.append(total)
        return jnp.concatenate(sums, axis=1)

    def sum_drain(phase):
        for piece in range(PIECES):
            pair_copy(phase, piece).wait_send()
            for d in range(1, n_chip):
                chip_copy(phase, piece, d, chip).wait_send()

    def head_columns(queries):
        blocks = [
            queries[:, h : h + HEAD].T for h in range(0, queries.shape[1], HEAD)
        ]
        return jnp.concatenate(blocks, axis=1).astype(BF16)

    def head_rows(columns):
        blocks = [
            columns[:, c : c + block_rows].T for c in range(0, columns.shape[1], block_rows)
        ]
        return jnp.concatenate(blocks, axis=1).astype(BF16)

    loads[0].wait()
    vectors["pre_first"].wait()
    with SC("norm0"):
        gather_start(0, normed(target_v[...], pre_first[...]))

    def src_copy(slot, c, device, kind):
        return to_tp(
            src.at[slot, c], src.at[slot, c], src_send.at[kind], src_recv.at[slot, c], device
        )

    loads[1].wait()
    vectors["source_gain"].wait()
    for c in range(CHUNKS):
        src[me, c] = normed(source_v[pl.ds(c * chunk, chunk)], source_gain[...]).astype(BF16)
        for d in range(1, n_chip):
            src_copy(me, c, tp_at(2 * d), 0).start()
        src_copy(me, c, sib, 0).start()

    def project_pair(block, c, mine, other, layers=(0, 1)):
        lines = jnp.concatenate([src[mine, c], src[other, c]], axis=0)
        place = pl.ds(c * 2 * chunk, 2 * chunk)
        if 0 in layers:
            first = dot(lines, keyval_first[...])
            k_first[block, place] = first[:, :HEAD].astype(BF16)
            v_first[block, place] = first[:, HEAD:].astype(BF16)
        if 1 in layers:
            second = dot(lines, keyval_second[...])
            kv_second[z, block, c, 0] = second[:, :HEAD].astype(BF16)
            kv_second[z, block, c, 1] = second[:, HEAD:].astype(BF16)

    def absorb(keys, values, queries, slot, fresh):
        absorb_scores(dot(keys, queries), values, slot, fresh)

    def absorb_scores(scores, values, slot, fresh):
        newest = jnp.max(scores, axis=0, keepdims=True)
        if not fresh:
            newest = jnp.maximum(newest, run_max[slot])
        weights = jnp.exp2((scores - newest) * EXP_SCALE)
        added = jnp.sum(weights, axis=0, keepdims=True)
        gathered = lax.dot_general(
            values, weights.astype(BF16), (((0,), (0,)), ((), ())), preferred_element_type=F32
        )
        if not fresh:
            rescale = jnp.exp2((run_max[slot] - newest) * EXP_SCALE)
            added = added + run_sum[slot] * rescale
            gathered = gathered + run_out[slot] * rescale
        run_max[slot] = newest
        run_sum[slot] = added
        run_out[slot] = gathered

    def absorb_block(block, fresh):
        @pl.loop(0, n_sp)
        def _(slot):
            absorb(k_first[block], v_first[block], q_slots[slot], slot, fresh)

    def kv_copy(block, slot, c, peer):
        held = kv_second.at[slot, block, c]
        return to_sp(held, held, kv_send, kv_recv.at[slot, block, c], peer)

    def kv_hop(block, hop, arrive=True, chunks=range(CHUNKS)):
        for step in (1, -1):
            slot = z - step * (hop - 1)
            peer = z + step

            @pl.when(jnp.logical_and(slot >= 0, slot < n_sp))
            def _():
                if arrive:
                    for c in chunks:
                        kv_copy(block, slot, c, sp_at(1)).wait_recv()

                @pl.when(jnp.logical_and(hop < n_sp, jnp.logical_and(peer >= 0, peer < n_sp)))
                def _():
                    for c in chunks:
                        kv_copy(block, slot, c, peer).start()

    def kv_drain(block, hop):
        for step in (1, -1):
            slot = z - step * (hop - 1)
            peer = z + step
            inside = jnp.logical_and(slot >= 0, slot < n_sp)

            @pl.when(jnp.logical_and(inside, jnp.logical_and(peer >= 0, peer < n_sp)))
            def _():
                for c in range(CHUNKS):
                    kv_copy(block, slot, c, peer).wait_send()

    def nearest(j):
        up = j + jnp.where(j >= z, 1, 0)
        down = n_sp - 1 - j
        down = down - jnp.where(down <= z, 1, 0)
        return jnp.where(2 * z < n_sp, up, down)

    def second_rows(slot, part):
        return kv_second[slot, :, :, part].reshape(n_chip * CHUNKS * 2 * chunk, HEAD)

    loads[3].wait()
    loads[4].wait()
    with SC("proj_own"):
        for c in range(CHUNKS):
            src_copy(sib, c, sib, 0).wait_recv()
            project_pair(0, c, me, sib)
    kv_hop(0, 1, False, range(CHUNKS // 2))
    loads[2].wait()
    with SC("qproj"):
        q_slots[z] = head_columns(gather_times(0, [query_first])[0])

    def q_copy(distance, slot):
        return to_sp(
            q_slots.at[z], q_slots.at[z] if slot is None else q_slots.at[slot],
            q_sem.at[0, 0], q_sem.at[1, z if slot is None else slot], sp_at(distance),
        )

    for d in range(1, n_sp):
        q_copy(d, None).start()

    last = n_chip - 1
    lead = CHUNKS // 2

    def near_chunk(d, c):
        near = tp_at(2 * d)
        src_copy(near, c, sib, 1).wait_recv()
        src_copy(near, c, sib, 1).start()

    def far_chunk(d, c, layers=(0, 1)):
        far = lax.rem(sib + 2 * d, n_tp)
        src_copy(far, c, sib, 1).wait_recv()
        project_pair(d, c, tp_at(2 * d), far, layers)

    def absorb_chunks(low, high):
        place = slice(low * 2 * chunk, high * 2 * chunk)

        @pl.loop(0, n_sp)
        def _(slot):
            absorb(k_first[last, place], v_first[last, place], q_slots[slot], slot, False)

    def lead_chunks():
        for c in range(lead):
            near_chunk(last, c)
            far_chunk(last, c)

    if n_chip == 2:
        with SC("lead"):
            lead_chunks()
    with SC("qwait"):
        for d in range(1, n_sp):
            q_copy(d, sp_at(d)).wait_recv()
    kv_hop(0, 1, False, range(lead, CHUNKS))
    kv_hop(0, 2, True, range(lead))
    with SC("abs_own"):
        absorb_block(0, True)

    def far_absorb(d):
        for c in range(CHUNKS):
            near_chunk(d, c)
            far_chunk(d, c)
        absorb_block(d, False)

    times(1, last, far_absorb)
    if n_chip > 2:
        lead_chunks()
    kv_hop(last, 1, False, range(lead))
    for c in range(lead, CHUNKS - 1):
        with SC("near"):
            near_chunk(last, c)
        with SC("abs_early"):
            absorb_chunks(0 if c == lead else c - 1, c)
        with SC("far"):
            far_chunk(last, c)
        kv_hop(last, 1, False, (c,))
    with SC("abs_early2"):
        absorb_chunks(CHUNKS - 2, CHUNKS - 1)
    with SC("near_last"):
        near_chunk(last, CHUNKS - 1)
    with SC("far_last"):
        far_chunk(last, CHUNKS - 1, (0,))
    early = (CHUNKS - 1) * 2 * chunk

    def mix_copies(peer, slot):
        return [
            to_sp(sent.at[peer], got.at[slot], mix_sem.at[index, 0, 0], mix_sem.at[index, 1, slot], peer)
            for index, (sent, got) in enumerate(((mix_send, mix_recv), (stat_send, stat_recv)))
        ]

    def finish_slot(slot):
        absorb(k_first[last, early:], v_first[last, early:], q_slots[slot], slot, False)

    def pack(peer):
        total = run_sum[peer]
        mix_send[peer] = (run_out[peer] / total).astype(BF16)
        stat_send[peer] = jnp.concatenate([run_max[peer], total], axis=0)

    def finish_and_send(peer):
        finish_slot(peer)
        pack(peer)
        for copy in mix_copies(peer, z):
            copy.start()

    relayed = n_sp > 2
    end = n_sp - 1
    gives, merges, takes = z == 0, z == 1, z == end

    def relay_copies():
        return [
            to_sp(sent.at[end], got, relay_sem.at[index, 0], relay_sem.at[index, 1], 1)
            for index, (sent, got) in enumerate(((mix_send, relay_mix), (stat_send, relay_stat)))
        ]

    def mix_order(j):
        return jnp.where(
            merges, jnp.where(j == n_sp - 2, end, nearest(n_sp - 2 - j - 1)), nearest(n_sp - 2 - j)
        )

    if relayed:

        @pl.loop(0, n_sp - 1)
        def _(j):
            peer = mix_order(j)
            finish_slot(peer)

            @pl.when(jnp.logical_not(jnp.logical_and(merges, peer == end)))
            def _():
                pack(peer)

                @pl.when(jnp.logical_and(gives, peer == end))
                def _():
                    for copy in relay_copies():
                        copy.start()

                @pl.when(jnp.logical_not(jnp.logical_and(gives, peer == end)))
                def _():
                    for copy in mix_copies(peer, z):
                        copy.start()

    else:

        @pl.loop(0, n_sp - 1)
        def _(j):
            finish_and_send(nearest(n_sp - 2 - j))

    with SC("finish_me"):
        finish_slot(z)
        project_pair(last, CHUNKS - 1, tp_at(2 * last), lax.rem(sib + 2 * last, n_tp), (1,))
    with SC("transpose"):
        loads[6].wait()
        loads[7].wait()
        for name in list(vectors)[2:]:
            vectors[name].wait()
        stripe = 2 * HEAD

        @pl.loop(0, width // stripe)
        def _(index):
            place = pl.ds(pl.multiple_of(index * stripe, stripe), stripe)
            w_gate[place, :] = gate_t[:, place].T
            w_value[place, :] = value_t[:, place].T

    def merge_into(slot, values, newest, count):
        top = jnp.maximum(newest, run_max[slot])
        rescale = jnp.exp2((run_max[slot] - top) * EXP_SCALE)
        share = jnp.exp2((newest - top) * EXP_SCALE) * count
        run_max[slot] = top
        run_sum[slot] = run_sum[slot] * rescale + share
        run_out[slot] = run_out[slot] * rescale + values.astype(F32) * share

    def merge(slot):
        for copy in mix_copies(slot, slot):
            copy.wait_recv()
        merge_into(z, mix_recv[slot], stat_recv[slot, 0:1], stat_recv[slot, 1:2])

    if relayed:
        with SC("relay"):

            @pl.when(merges)
            def _():
                for copy in relay_copies():
                    copy.wait_recv()
                merge_into(end, relay_mix[...], relay_stat[0:1], relay_stat[1:2])
                pack(end)
                for copy in mix_copies(end, z):
                    copy.start()

    with SC("mixwait"):
        @pl.loop(0, n_sp - 1)
        def _(j):
            slot = nearest(j)

            @pl.when(jnp.logical_not(jnp.logical_and(takes, slot == 0) if relayed else z < 0))
            def _():
                merge(slot)

    with SC("kv_a"):
        kv_hop(last, 1, False, (CHUNKS - 1,))
        for block in range(1, last):
            kv_hop(block, 1, False)
        kv_hop(0, 2, True, range(lead, CHUNKS))
        kv_hop(last, 2, True, range(CHUNKS - 1))
    loads[5].wait()
    with SC("rs0"):
        mixed = scatter_sum(0, head_rows(run_out[z] / run_sum[z]), out_first)
    after_first = target_v[...].astype(F32) + normed(mixed, post_first[...])
    stream[...] = after_first

    def halo_copy(device):
        return pltpu.make_async_remote_copy(
            src_ref=halo_send, dst_ref=halo_recv, send_sem=halo_sem.at[0],
            recv_sem=halo_sem.at[1], device_id=device, device_id_type=MESH,
        )

    ffn_input = normed(after_first, ffn_pre[...])

    @pl.when(gives_halo)
    def _():
        halo_send[...] = ffn_input[rows - 2 :].astype(BF16)
        for t in range(n_tp):
            halo_copy({"sp": z + 1, "tp": t}).start()

    gather_start(1, ffn_input)
    with SC("kv_b"):
        for block in range(1, last):
            kv_hop(block, 2)
        kv_hop(0, 3, True, range(lead))
        kv_hop(last, 2, True, (CHUNKS - 1,))

    def halo_rows():
        @pl.when(z > 0)
        def _():
            halo_copy({"sp": z, "tp": sib}).wait_recv()

        zeros = jnp.zeros((14, width), F32)
        return jnp.concatenate([halo_recv[...].astype(F32), zeros], axis=0).astype(BF16)

    with SC("ag1_up"):
        up_gate, up_value = (
            up.astype(BF16) for up in gather_times(1, [w_gate, w_value], halo_rows)
        )

    def causal_mix(up_rows, taps):
        here = up_rows[:block_rows].astype(F32)
        rim = jnp.where(z > 0, up_rows[block_rows:].astype(F32), 0.0)
        row = lax.broadcasted_iota(jnp.int32, here.shape, 0)
        before = jnp.where(row == 0, rim[1:2], pltpu.roll(here, 1, 0))
        earlier = jnp.where(
            row == 0, rim[0:1], jnp.where(row == 1, rim[1:2], pltpu.roll(here, 2, 0))
        )
        return taps[0:1] * earlier + taps[1:2] * before + taps[2:3] * here

    with SC("gated"):
        gated = (
            jax.nn.gelu(causal_mix(up_gate, conv_gate[...]), approximate=True)
            * causal_mix(up_value, conv_value[...])
        ).astype(BF16)
        loads[8].wait()
    with SC("kv_c"):
        kv_hop(0, 3, True, range(lead, CHUNKS))
        kv_hop(last, 3, True, range(CHUNKS - 1))
    with SC("rs1"):
        ffn_sum = scatter_sum(1, gated, w_down)
    after_ffn = stream[...] + normed(ffn_sum, ffn_post[...])
    stream[...] = after_ffn

    gather_start(2, normed(after_ffn, pre_second[...]))
    with SC("kv_d"):
        for block in range(1, last):
            kv_hop(block, 3)
        kv_hop(last, 3, True, (CHUNKS - 1,))
    with SC("ag2_q"):
        loads[9].wait()
        queries = head_columns(gather_times(2, [query_second])[0])
        for d in range(1, n_sp):
            q_copy(d, None).wait_send()
        q_slots[z] = queries

    def kv_rest():
        @pl.loop(4, max(n_sp, 4) + 1)
        def _(hop):
            for block in range(n_chip):
                kv_hop(block, hop)

    def absorb_second(j):
        slot = nearest(j)
        absorb(second_rows(slot, 0), second_rows(slot, 1), q_slots[z], 0, False)

    with SC("attn2"):
        if n_sp > 4:
            absorb(second_rows(z, 0), second_rows(z, 1), q_slots[z], 0, True)
            kv_rest()
            times(0, n_sp - 1, absorb_second)
        else:
            slots = [z] + [nearest(j) for j in range(n_sp - 1)]
            scores = dot(second_rows(z, 0), q_slots[z])
            for index, slot in enumerate(slots):
                if index == n_sp - 2:
                    kv_rest()
                if index < n_sp - 1:
                    ahead = dot(second_rows(slots[index + 1], 0), q_slots[z])
                absorb_scores(scores, second_rows(slot, 1), 0, index == 0)
                scores = ahead

    with SC("rs2"):
        loads[10].wait()
        mixed = scatter_sum(2, head_rows(run_out[0] / run_sum[0]), out_second)
    decoded[...] = stream[...] + normed(mixed, post_second[...])

    for phase in range(3):
        gather_drain(phase)
        sum_drain(phase)
    for c in range(CHUNKS):
        for _ in range(n_chip):
            src_copy(me, c, sib, 0).wait_send()
        for d in range(1, n_chip):
            src_copy(me, c, sib, 1).wait_send()

    def drain(d):
        for block in range(n_chip):
            kv_drain(block, d)
        relay = jnp.logical_and(gives, sp_at(d) == end) if relayed else z < 0

        @pl.when(jnp.logical_not(relay))
        def _():
            for copy in mix_copies(sp_at(d), z):
                copy.wait_send()

    times(1, n_sp, drain)
    if relayed:

        @pl.when(gives)
        def _():
            for copy in relay_copies():
                copy.wait_send()

    @pl.when(gives_halo)
    def _():
        for t in range(n_tp):
            halo_copy({"sp": z, "tp": sib}).wait_send()


def per_device(*arrays):
    (target, source, source_gain, pre_first, query_first, keyval_first, out_first, post_first,
     ffn_pre, w_gate, w_value, conv_gate, conv_value, w_down, ffn_post, pre_second,
     query_second, keyval_second, out_second, post_second) = arrays
    n_tp, n_sp = lax.axis_size("tp"), lax.axis_size("sp")
    sharers = 2 * HEAD // keyval_first.shape[1]
    if sharers > 1:
        groups = [list(range(low, low + sharers)) for low in range(0, n_tp, sharers)]
        keyval_first, keyval_second = (
            lax.all_gather(w, "tp", axis=1, tiled=True, axis_index_groups=groups)
            for w in (keyval_first, keyval_second)
        )
    rows, width = target.shape
    lines = source.shape[0]
    block_rows = rows * n_tp
    columns = query_first.shape[1] // HEAD * block_rows
    n_chip = n_tp // 2
    span = width // PIECES
    dma = pltpu.SemaphoreType.DMA
    hbm = pl.BlockSpec(memory_space=pltpu.HBM)
    vmem = pl.BlockSpec(memory_space=pltpu.VMEM)

    def row(gain):
        return gain.reshape(1, width)

    line = pltpu.VMEM((1, width), F32)
    scratch = [
        *([line] * 4), pltpu.VMEM(conv_gate.shape, F32), pltpu.VMEM(conv_value.shape, F32),
        *([line] * 3), dma((9,)),
        pltpu.VMEM(target.shape, BF16),
        pltpu.VMEM(source.shape, BF16),
        *(pltpu.VMEM(w.shape, BF16) for w in (
            query_first, keyval_first, out_first, w_gate.T, w_value.T, w_gate, w_value, w_down,
            query_second, keyval_second, out_second)),
        dma((11,)),
        pltpu.VMEM((3, PIECES, n_tp, rows, span), BF16),
        dma((3,)),
        dma((3, PIECES, n_tp)),
        pltpu.VMEM((n_tp, CHUNKS, lines // CHUNKS, width), BF16),
        dma((2,)),
        dma((n_tp, CHUNKS)),
        pltpu.VMEM((n_sp, HEAD, columns), BF16),
        dma((2, n_sp)),
        pltpu.VMEM((n_chip, 2 * lines, HEAD), BF16),
        pltpu.VMEM((n_chip, 2 * lines, HEAD), BF16),
        pltpu.VMEM((n_sp, n_chip, CHUNKS, 2, 2 * lines // CHUNKS, HEAD), BF16),
        dma,
        dma((n_sp, n_chip, CHUNKS)),
        pltpu.VMEM((n_sp, 1, columns), F32),
        pltpu.VMEM((n_sp, 1, columns), F32),
        pltpu.VMEM((n_sp, HEAD, columns), F32),
        pltpu.VMEM((n_sp, HEAD, columns), BF16),
        pltpu.VMEM((n_sp, HEAD, columns), BF16),
        pltpu.VMEM((n_sp, 2, columns), F32),
        pltpu.VMEM((n_sp, 2, columns), F32),
        dma((2, 2, n_sp)),
        pltpu.VMEM((3, PIECES, 2, n_chip, rows, span), BF16),
        pltpu.VMEM((3, PIECES, n_chip, rows, span), BF16),
        pltpu.VMEM((3, PIECES, n_chip, rows, span), BF16),
        pltpu.VMEM((3, PIECES, n_chip, rows, span), BF16),
        dma((3, 2)),
        dma((3, PIECES)),
        dma((3, PIECES, n_chip)),
        pltpu.VMEM((2, width), BF16),
        pltpu.VMEM((2, width), BF16),
        dma((2,)),
        pltpu.VMEM((rows, width), F32),
        pltpu.VMEM((HEAD, columns), BF16),
        pltpu.VMEM((2, columns), F32),
        dma((2, 2)),
    ]

    def kernel(*refs):
        decoder_kernel(n_tp, n_sp, *refs)

    return pl.pallas_call(
        kernel,
        out_shape=pltpu.VMEM((rows, width), F32),
        in_specs=[hbm] * 20,
        out_specs=vmem,
        scratch_shapes=scratch,
        compiler_params=pltpu.CompilerParams(
            collective_id=0, has_side_effects=True, vmem_limit_bytes=60_000_000
        ),
        name="decoder",
    )(
        target, source, row(source_gain), row(pre_first), query_first, keyval_first, out_first,
        row(post_first), row(ffn_pre), w_gate.T, w_value.T, conv_gate, conv_value, w_down,
        row(ffn_post), row(pre_second), query_second, keyval_second, out_second, row(post_second),
    )


def solution(mesh):
    rows = P(("grp", "sp", "tp"), None)
    by_column, by_row = P(None, "tp"), P("tp", None)
    placed = (
        rows, rows, P(), P(), by_column, by_column, by_row, P(), P(), by_column, by_column,
        by_column, by_column, by_row, P(), P(), by_column, by_column, by_row, P(),
    )
    return jax.shard_map(
        per_device, mesh=mesh, in_specs=placed, out_specs=rows, check_vma=False
    )
```

```python
import math

import jax
import jax.numpy as jnp
from jax import lax
from jax.experimental import pallas as pl
from jax.experimental.pallas import tpu as pltpu
from jax.sharding import PartitionSpec as P

HEAD = 128
CHUNKS = 4
PIECES = 2
EXP_SCALE = HEAD ** (-0.5) * math.log2(math.e)
F32, BF16 = jnp.float32, jnp.bfloat16
MESH = pl.DeviceIdType.MESH


def normed(values, gain):
    widened = values.astype(F32)
    return widened * lax.rsqrt(jnp.mean(widened * widened, axis=-1, keepdims=True) + 1e-06) * gain


SC = jax.named_scope


def times(start, stop, body):
    if stop - start <= 4:
        for index in range(start, stop):
            body(index)
    else:

        @pl.loop(start, stop)
        def _(index):
            body(index)


def dot(left, right):
    return jnp.dot(left, right, preferred_element_type=F32)


def decoder_kernel(
    n_tp,
    n_sp,
    target_h,
    source_h,
    source_gain_h,
    pre_first_h,
    query_first_h,
    keyval_first_h,
    out_first_h,
    post_first_h,
    ffn_pre_h,
    gate_h,
    value_h,
    conv_gate_h,
    conv_value_h,
    down_h,
    ffn_post_h,
    pre_second_h,
    query_second_h,
    keyval_second_h,
    out_second_h,
    post_second_h,
    decoded,
    source_gain,
    pre_first,
    post_first,
    ffn_pre,
    conv_gate,
    conv_value,
    ffn_post,
    pre_second,
    post_second,
    target_v,
    source_v,
    query_first,
    keyval_first,
    out_first,
    gate_t,
    value_t,
    w_gate,
    w_value,
    w_down,
    query_second,
    keyval_second,
    out_second,
    local_sem,
    hidden,
    hidden_send,
    hidden_recv,
    src,
    src_send,
    src_recv,
    q_slots,
    q_sem,
    k_first,
    v_first,
    kv_second,
    kv_send,
    kv_recv,
    run_max,
    run_sum,
    run_out,
    mix_send,
    mix_recv,
    stat_send,
    stat_recv,
    mix_sem,
    part,
    pair_recv,
    pair_sum,
    part_recv,
    part_send,
    pair_sem,
    part_sem,
    halo_send,
    halo_recv,
    halo_sem,
    stream,
    relay_mix,
    relay_stat,
    relay_sem,
):
    me = lax.axis_index("tp")
    z = lax.axis_index("sp")
    sib = me + 1 - 2 * lax.rem(me, 2)
    core, chip = lax.rem(me, 2), me // 2
    n_chip = n_tp // 2
    rows = target_v.shape[0]
    width = target_v.shape[1]
    span = width // PIECES
    chunk = src.shape[2]
    block_rows = rows * n_tp

    def tp_at(distance):
        return lax.rem(me + distance, n_tp)

    def sp_at(distance):
        return lax.rem(z + distance, n_sp)

    def to_tp(source, dest, send, recv, device):
        return pltpu.make_async_remote_copy(
            src_ref=source, dst_ref=dest, send_sem=send, recv_sem=recv,
            device_id={"tp": device}, device_id_type=MESH,
        )

    def to_sp(source, dest, send, recv, device):
        return pltpu.make_async_remote_copy(
            src_ref=source, dst_ref=dest, send_sem=send, recv_sem=recv,
            device_id={"sp": device}, device_id_type=MESH,
        )

    pairs = [
        (target_h, target_v),
        (source_h, source_v),
        (query_first_h, query_first),
        (keyval_first_h, keyval_first),
        (keyval_second_h, keyval_second),
        (out_first_h, out_first),
        (gate_h, gate_t),
        (value_h, value_t),
        (down_h, w_down),
        (query_second_h, query_second),
        (out_second_h, out_second),
    ]
    loads = [
        pltpu.make_async_copy(a, b, local_sem.at[i])
        for i, (a, b) in enumerate(pairs)
    ]
    vectors = {
        name: pltpu.make_async_copy(a, b, local_sem.at[len(pairs) + i])
        for i, (name, a, b) in enumerate([
            ("pre_first", pre_first_h, pre_first),
            ("source_gain", source_gain_h, source_gain),
            ("post_first", post_first_h, post_first),
            ("ffn_pre", ffn_pre_h, ffn_pre),
            ("conv_gate", conv_gate_h, conv_gate),
            ("conv_value", conv_value_h, conv_value),
            ("ffn_post", ffn_post_h, ffn_post),
            ("pre_second", pre_second_h, pre_second),
            ("post_second", post_second_h, post_second),
        ])
    }
    loads[0].start()
    vectors["pre_first"].start()
    vectors["source_gain"].start()
    for load in loads[1:]:
        load.start()
    for name in list(vectors)[2:]:
        vectors[name].start()

    barrier = pltpu.get_barrier_semaphore()
    for distance in range(1, n_tp):
        pl.semaphore_signal(barrier, inc=1, device_id={"tp": tp_at(distance)}, device_id_type=MESH)
    for distance in range(1, n_sp):
        pl.semaphore_signal(barrier, inc=1, device_id={"sp": sp_at(distance)}, device_id_type=MESH)
    last_tp = n_tp - 1

    @pl.when(jnp.logical_and(z > 0, me < last_tp))
    def _():
        pl.semaphore_signal(
            barrier, inc=1, device_id={"sp": z - 1, "tp": last_tp}, device_id_type=MESH
        )

    gives_halo = jnp.logical_and(me == last_tp, z < n_sp - 1)
    with SC("barrier"):
        pl.semaphore_wait(barrier, n_tp - 1 + n_sp - 1 + jnp.where(gives_halo, n_tp - 1, 0))

    def hidden_copy(phase, piece, slot, device, index=0):
        return to_tp(
            hidden.at[phase, piece, slot], hidden.at[phase, piece, slot],
            hidden_send, hidden_recv.at[phase, piece, index], device,
        )

    def gather_start(phase, value):
        for piece in range(PIECES):
            hidden[phase, piece, me] = value[:, piece * span : (piece + 1) * span].astype(BF16)
            for d in range(1, n_chip):
                hidden_copy(phase, piece, me, tp_at(2 * d), n_chip - d).start()
            hidden_copy(phase, piece, me, sib).start()

    def gather_times(phase, weights, extra=None):
        totals = [None] * len(weights)
        for piece in range(PIECES + 1):
            if piece < PIECES:
                for d in range(1, n_chip):
                    slot = tp_at(2 * d)
                    hidden_copy(phase, piece, slot, sib, d).wait_recv()
                    hidden_copy(phase, piece, slot, sib).start()
            if piece == 0:
                continue
            ready = piece - 1
            both = hidden.at[phase, ready, pl.ds(0, n_chip)]
            pltpu.make_async_copy(both, both, hidden_recv.at[phase, ready, 0]).wait()
            whole = hidden[phase, ready]
            if rows % 16:
                whole = whole.astype(F32).reshape(block_rows, span).astype(BF16)
            else:
                whole = whole.reshape(block_rows, span)
            if extra is not None:
                if ready == 0:
                    rim = extra()
                whole = jnp.concatenate([whole, rim[:, ready * span : (ready + 1) * span]], axis=0)
            for index, weight in enumerate(weights):
                product = dot(whole, weight[ready * span : (ready + 1) * span, :])
                totals[index] = product if ready == 0 else totals[index] + product
        return totals

    def gather_drain(phase):
        for piece in range(PIECES):
            for _ in range(2 * n_chip - 1):
                hidden_copy(phase, piece, me, sib).wait_send()

    def pair_copy(phase, piece):
        return to_tp(
            part.at[phase, piece, 1 - core], pair_recv.at[phase, piece],
            part_send.at[0], pair_sem.at[phase, piece], sib,
        )

    def chip_copy(phase, piece, distance, slot, index):
        other = lax.rem(chip + distance, n_chip)
        return to_tp(
            pair_sum.at[phase, piece, other], part_recv.at[phase, piece, slot],
            part_send.at[1], part_sem.at[phase, piece, index], 2 * other + core,
        )

    def scatter_sum(phase, left, weight):
        for piece in range(PIECES):
            product = dot(left, weight[:, piece * span : (piece + 1) * span])
            product = product.reshape(n_chip, 2, rows, span)
            for parity in range(2):
                part[phase, piece, parity] = product[:, parity].astype(BF16)
            pair_copy(phase, piece).start()
        for piece in range(PIECES):
            pair_copy(phase, piece).wait_recv()
            mine = part[phase, piece, core].astype(F32)
            pair_sum[phase, piece] = (mine + pair_recv[phase, piece].astype(F32)).astype(BF16)
            for d in range(1, n_chip):
                chip_copy(phase, piece, d, chip, n_chip - d - 1).start()
        sums = []
        for piece in range(PIECES):
            total = pair_sum[phase, piece, chip].astype(F32)
            for d in range(1, n_chip):
                slot = lax.rem(chip + d, n_chip)
                chip_copy(phase, piece, d, slot, d - 1).wait_recv()
                total = total + part_recv[phase, piece, slot].astype(F32)
            sums.append(total)
        return jnp.concatenate(sums, axis=1)

    def sum_drain(phase):
        for piece in range(PIECES):
            pair_copy(phase, piece).wait_send()
            for d in range(1, n_chip):
                chip_copy(phase, piece, d, chip, d - 1).wait_send()

    def head_columns(queries):
        blocks = [
            queries[:, h : h + HEAD].T for h in range(0, queries.shape[1], HEAD)
        ]
        return jnp.concatenate(blocks, axis=1).astype(BF16)

    def head_rows(columns):
        blocks = [
            columns[:, c : c + block_rows].T for c in range(0, columns.shape[1], block_rows)
        ]
        return jnp.concatenate(blocks, axis=1).astype(BF16)

    loads[0].wait()
    vectors["pre_first"].wait()
    with SC("norm0"):
        gather_start(0, normed(target_v[...], pre_first[...]))

    def src_copy(slot, c, device, index):
        return to_tp(src.at[slot, c], src.at[slot, c], src_send, src_recv.at[index, c], device)

    loads[1].wait()
    vectors["source_gain"].wait()
    for c in range(CHUNKS):
        src[me, c] = normed(source_v[pl.ds(c * chunk, chunk)], source_gain[...]).astype(BF16)
        for d in range(1, n_chip):
            src_copy(me, c, tp_at(2 * d), n_chip - d).start()
        src_copy(me, c, sib, 0).start()

    def project_pair(block, c, mine, other, layers=(0, 1)):
        lines = jnp.concatenate([src[mine, c], src[other, c]], axis=0)
        place = pl.ds(c * 2 * chunk, 2 * chunk)
        if 0 in layers:
            first = dot(lines, keyval_first[...])
            k_first[block, place] = first[:, :HEAD].astype(BF16)
            v_first[block, place] = first[:, HEAD:].astype(BF16)
        if 1 in layers:
            second = dot(lines, keyval_second[...])
            kv_second[z, block, c, 0] = second[:, :HEAD].astype(BF16)
            kv_second[z, block, c, 1] = second[:, HEAD:].astype(BF16)

    def absorb(keys, values, queries, slot, fresh):
        absorb_scores(dot(keys, queries), values, slot, fresh)

    def absorb_scores(scores, values, slot, fresh):
        newest = jnp.max(scores, axis=0, keepdims=True)
        if not fresh:
            newest = jnp.maximum(newest, run_max[slot])
        weights = jnp.exp2((scores - newest) * EXP_SCALE)
        added = jnp.sum(weights, axis=0, keepdims=True)
        gathered = lax.dot_general(
            values, weights.astype(BF16), (((0,), (0,)), ((), ())), preferred_element_type=F32
        )
        if not fresh:
            rescale = jnp.exp2((run_max[slot] - newest) * EXP_SCALE)
            added = added + run_sum[slot] * rescale
            gathered = gathered + run_out[slot] * rescale
        run_max[slot] = newest
        run_sum[slot] = added
        run_out[slot] = gathered

    def absorb_block(block, fresh):
        @pl.loop(0, n_sp)
        def _(slot):
            absorb(k_first[block], v_first[block], q_slots[slot], slot, fresh)

    last = n_chip - 1
    lead = CHUNKS // 2

    def kv_copy(block, slot, c, peer, receiver):
        held = kv_second.at[slot, block, c]
        index = slot - jnp.where(slot > receiver, 1, 0)
        group = int(c >= (lead if block == 0 else CHUNKS - 1))
        return to_sp(held, held, kv_send, kv_recv.at[index, block, group], peer)

    def kv_wait(block, slot, chunks):
        edge = lead if block == 0 else CHUNKS - 1
        index = slot - jnp.where(slot > z, 1, 0)
        for group in range(2):
            count = sum(int(c >= edge) == group for c in chunks)
            if count:
                held = kv_second.at[slot, block, pl.ds(edge * group, count)]
                pltpu.make_async_copy(held, held, kv_recv.at[index, block, group]).wait()

    def kv_hop(block, hop, arrive=True, chunks=range(CHUNKS)):
        for step in (1, -1):
            slot = z - step * (hop - 1)
            peer = z + step

            @pl.when(jnp.logical_and(slot >= 0, slot < n_sp))
            def _():
                if arrive:
                    kv_wait(block, slot, chunks)

                @pl.when(jnp.logical_and(hop < n_sp, jnp.logical_and(peer >= 0, peer < n_sp)))
                def _():
                    for c in chunks:
                        kv_copy(block, slot, c, peer, peer).start()

    def kv_drain(block, hop):
        for step in (1, -1):
            slot = z - step * (hop - 1)
            peer = z + step
            inside = jnp.logical_and(slot >= 0, slot < n_sp)

            @pl.when(jnp.logical_and(inside, jnp.logical_and(peer >= 0, peer < n_sp)))
            def _():
                for c in range(CHUNKS):
                    kv_copy(block, slot, c, peer, peer).wait_send()

    def nearest(j):
        up = j + jnp.where(j >= z, 1, 0)
        down = n_sp - 1 - j
        down = down - jnp.where(down <= z, 1, 0)
        return jnp.where(2 * z < n_sp, up, down)

    def second_rows(slot, part):
        return kv_second[slot, :, :, part].reshape(n_chip * CHUNKS * 2 * chunk, HEAD)

    loads[3].wait()
    loads[4].wait()
    with SC("proj_own"):
        for c in range(CHUNKS):
            src_copy(sib, c, sib, 0).wait_recv()
            project_pair(0, c, me, sib)
    kv_hop(0, 1, False, range(CHUNKS // 2))
    loads[2].wait()
    with SC("qproj"):
        q_slots[z] = head_columns(gather_times(0, [query_first])[0])

    def q_copy(distance, slot):
        return to_sp(
            q_slots.at[z], q_slots.at[z] if slot is None else q_slots.at[slot],
            q_sem.at[0], q_sem.at[1], sp_at(distance),
        )

    for d in range(1, n_sp):
        q_copy(d, None).start()


    def near_chunk(d, c):
        near = tp_at(2 * d)
        src_copy(near, c, sib, d).wait_recv()
        src_copy(near, c, sib, n_chip - 1 + d).start()

    def far_chunk(d, c, layers=(0, 1)):
        far = lax.rem(sib + 2 * d, n_tp)
        src_copy(far, c, sib, n_chip - 1 + d).wait_recv()
        project_pair(d, c, tp_at(2 * d), far, layers)

    def absorb_chunks(low, high):
        place = slice(low * 2 * chunk, high * 2 * chunk)

        @pl.loop(0, n_sp)
        def _(slot):
            absorb(k_first[last, place], v_first[last, place], q_slots[slot], slot, False)

    def lead_chunks():
        for c in range(lead):
            near_chunk(last, c)
            far_chunk(last, c)

    if n_chip == 2:
        with SC("lead"):
            lead_chunks()
    with SC("qwait"):
        others = q_slots.at[pl.ds(0, n_sp - 1)]
        pltpu.make_async_copy(others, others, q_sem.at[1]).wait()
    kv_hop(0, 1, False, range(lead, CHUNKS))
    kv_hop(0, 2, True, range(lead))
    with SC("abs_own"):
        absorb_block(0, True)

    def far_absorb(d):
        for c in range(CHUNKS):
            near_chunk(d, c)
            far_chunk(d, c)
        absorb_block(d, False)

    times(1, last, far_absorb)
    if n_chip > 2:
        lead_chunks()
    kv_hop(last, 1, False, range(lead))
    for c in range(lead, CHUNKS - 1):
        with SC("near"):
            near_chunk(last, c)
        with SC("abs_early"):
            absorb_chunks(0 if c == lead else c - 1, c)
        with SC("far"):
            far_chunk(last, c)
        kv_hop(last, 1, False, (c,))
    with SC("abs_early2"):
        absorb_chunks(CHUNKS - 2, CHUNKS - 1)
    with SC("near_last"):
        near_chunk(last, CHUNKS - 1)
    with SC("far_last"):
        far_chunk(last, CHUNKS - 1, (0,))
    early = (CHUNKS - 1) * 2 * chunk

    def mix_copies(peer, slot):
        return [
            to_sp(sent.at[peer], got.at[slot], mix_sem.at[index, n_sp], mix_sem.at[index, slot], peer)
            for index, (sent, got) in enumerate(((mix_send, mix_recv), (stat_send, stat_recv)))
        ]

    def finish_slot(slot):
        absorb(k_first[last, early:], v_first[last, early:], q_slots[slot], slot, False)

    def pack(peer):
        total = run_sum[peer]
        mix_send[peer] = (run_out[peer] / total).astype(BF16)
        stat_send[peer] = jnp.concatenate([run_max[peer], total], axis=0)

    def finish_and_send(peer):
        finish_slot(peer)
        pack(peer)
        for copy in mix_copies(peer, z):
            copy.start()

    relayed = n_sp > 2
    end = n_sp - 1
    gives, merges, takes = z == 0, z == 1, z == end

    def relay_copies():
        return [
            to_sp(sent.at[end], got, relay_sem.at[index, 0], relay_sem.at[index, 1], 1)
            for index, (sent, got) in enumerate(((mix_send, relay_mix), (stat_send, relay_stat)))
        ]

    def mix_order(j):
        return jnp.where(
            merges, jnp.where(j == n_sp - 2, end, nearest(n_sp - 2 - j - 1)), nearest(n_sp - 2 - j)
        )

    if relayed:

        @pl.loop(0, n_sp - 1)
        def _(j):
            peer = mix_order(j)
            finish_slot(peer)

            @pl.when(jnp.logical_not(jnp.logical_and(merges, peer == end)))
            def _():
                pack(peer)

                @pl.when(jnp.logical_and(gives, peer == end))
                def _():
                    for copy in relay_copies():
                        copy.start()

                @pl.when(jnp.logical_not(jnp.logical_and(gives, peer == end)))
                def _():
                    for copy in mix_copies(peer, z):
                        copy.start()

    else:

        @pl.loop(0, n_sp - 1)
        def _(j):
            finish_and_send(nearest(n_sp - 2 - j))

    with SC("finish_me"):
        finish_slot(z)
        project_pair(last, CHUNKS - 1, tp_at(2 * last), lax.rem(sib + 2 * last, n_tp), (1,))
    with SC("transpose"):
        for load in loads[5:]:
            load.wait()
        for name in list(vectors)[2:]:
            vectors[name].wait()
        stripe = 2 * HEAD

        @pl.loop(0, width // stripe)
        def _(index):
            place = pl.ds(pl.multiple_of(index * stripe, stripe), stripe)
            w_gate[place, :] = gate_t[:, place].T
            w_value[place, :] = value_t[:, place].T

    def merge_into(slot, values, newest, count):
        top = jnp.maximum(newest, run_max[slot])
        rescale = jnp.exp2((run_max[slot] - top) * EXP_SCALE)
        share = jnp.exp2((newest - top) * EXP_SCALE) * count
        run_max[slot] = top
        run_sum[slot] = run_sum[slot] * rescale + share
        run_out[slot] = run_out[slot] * rescale + values.astype(F32) * share

    def merge(slot):
        for copy in mix_copies(slot, slot):
            copy.wait_recv()
        merge_into(z, mix_recv[slot], stat_recv[slot, 0:1], stat_recv[slot, 1:2])

    if relayed:
        with SC("relay"):

            @pl.when(merges)
            def _():
                for copy in relay_copies():
                    copy.wait_recv()
                merge_into(end, relay_mix[...], relay_stat[0:1], relay_stat[1:2])
                pack(end)
                for copy in mix_copies(end, z):
                    copy.start()

    with SC("mixwait"):
        @pl.loop(0, n_sp - 1)
        def _(j):
            slot = nearest(j)

            @pl.when(jnp.logical_not(jnp.logical_and(takes, slot == 0) if relayed else z < 0))
            def _():
                merge(slot)

    with SC("kv_a"):
        kv_hop(last, 1, False, (CHUNKS - 1,))
        for block in range(1, last):
            kv_hop(block, 1, False)
        kv_hop(0, 2, True, range(lead, CHUNKS))
        kv_hop(last, 2, True, range(CHUNKS - 1))
    with SC("rs0"):
        mixed = scatter_sum(0, head_rows(run_out[z] / run_sum[z]), out_first)
    after_first = target_v[...].astype(F32) + normed(mixed, post_first[...])
    stream[...] = after_first

    def halo_copy(device):
        return pltpu.make_async_remote_copy(
            src_ref=halo_send, dst_ref=halo_recv, send_sem=halo_sem.at[0],
            recv_sem=halo_sem.at[1], device_id=device, device_id_type=MESH,
        )

    ffn_input = normed(after_first, ffn_pre[...])

    @pl.when(gives_halo)
    def _():
        halo_send[...] = ffn_input[rows - 2 :].astype(BF16)
        for t in range(n_tp):
            halo_copy({"sp": z + 1, "tp": t}).start()

    gather_start(1, ffn_input)
    with SC("kv_b"):
        for block in range(1, last):
            kv_hop(block, 2)
        kv_hop(0, 3, True, range(lead))
        kv_hop(last, 2, True, (CHUNKS - 1,))

    def halo_rows():
        @pl.when(z > 0)
        def _():
            halo_copy({"sp": z, "tp": sib}).wait_recv()

        zeros = jnp.zeros((14, width), F32)
        return jnp.concatenate([halo_recv[...].astype(F32), zeros], axis=0).astype(BF16)

    with SC("ag1_up"):
        up_gate, up_value = (
            up.astype(BF16) for up in gather_times(1, [w_gate, w_value], halo_rows)
        )

    def causal_mix(up_rows, taps):
        here = up_rows[:block_rows].astype(F32)
        rim = jnp.where(z > 0, up_rows[block_rows:].astype(F32), 0.0)
        row = lax.broadcasted_iota(jnp.int32, here.shape, 0)
        before = jnp.where(row == 0, rim[1:2], pltpu.roll(here, 1, 0))
        earlier = jnp.where(
            row == 0, rim[0:1], jnp.where(row == 1, rim[1:2], pltpu.roll(here, 2, 0))
        )
        return taps[0:1] * earlier + taps[1:2] * before + taps[2:3] * here

    with SC("gated"):
        gated = (
            jax.nn.gelu(causal_mix(up_gate, conv_gate[...]), approximate=True)
            * causal_mix(up_value, conv_value[...])
        ).astype(BF16)
    with SC("kv_c"):
        kv_hop(0, 3, True, range(lead, CHUNKS))
        kv_hop(last, 3, True, range(CHUNKS - 1))
    with SC("rs1"):
        ffn_sum = scatter_sum(1, gated, w_down)
    after_ffn = stream[...] + normed(ffn_sum, ffn_post[...])
    stream[...] = after_ffn

    gather_start(2, normed(after_ffn, pre_second[...]))
    with SC("kv_d"):
        for block in range(1, last):
            kv_hop(block, 3)
        kv_hop(last, 3, True, (CHUNKS - 1,))
    with SC("ag2_q"):
        queries = head_columns(gather_times(2, [query_second])[0])
        for d in range(1, n_sp):
            q_copy(d, None).wait_send()
        q_slots[z] = queries

    def kv_rest():
        @pl.loop(4, max(n_sp, 4) + 1)
        def _(hop):
            for block in range(n_chip):
                kv_hop(block, hop)

    def absorb_second(j):
        slot = nearest(j)
        absorb(second_rows(slot, 0), second_rows(slot, 1), q_slots[z], 0, False)

    with SC("attn2"):
        if n_sp > 4:
            absorb(second_rows(z, 0), second_rows(z, 1), q_slots[z], 0, True)
            kv_rest()
            times(0, n_sp - 1, absorb_second)
        else:
            slots = [z] + [nearest(j) for j in range(n_sp - 1)]
            scores = dot(second_rows(z, 0), q_slots[z])
            for index, slot in enumerate(slots):
                if index == n_sp - 2:
                    kv_rest()
                if index < n_sp - 1:
                    ahead = dot(second_rows(slots[index + 1], 0), q_slots[z])
                absorb_scores(scores, second_rows(slot, 1), 0, index == 0)
                scores = ahead

    with SC("rs2"):
        mixed = scatter_sum(2, head_rows(run_out[0] / run_sum[0]), out_second)
    decoded[...] = stream[...] + normed(mixed, post_second[...])

    for phase in range(3):
        gather_drain(phase)
        sum_drain(phase)
    for c in range(CHUNKS):
        for _ in range(n_chip):
            src_copy(me, c, sib, 0).wait_send()
        for d in range(1, n_chip):
            src_copy(me, c, sib, 1).wait_send()

    def drain(d):
        for block in range(n_chip):
            kv_drain(block, d)
        relay = jnp.logical_and(gives, sp_at(d) == end) if relayed else z < 0

        @pl.when(jnp.logical_not(relay))
        def _():
            for copy in mix_copies(sp_at(d), z):
                copy.wait_send()

    times(1, n_sp, drain)
    if relayed:

        @pl.when(gives)
        def _():
            for copy in relay_copies():
                copy.wait_send()

    @pl.when(gives_halo)
    def _():
        for t in range(n_tp):
            halo_copy({"sp": z, "tp": sib}).wait_send()


def per_device(*arrays):
    (target, source, source_gain, pre_first, query_first, keyval_first, out_first, post_first,
     ffn_pre, w_gate, w_value, conv_gate, conv_value, w_down, ffn_post, pre_second,
     query_second, keyval_second, out_second, post_second) = arrays
    n_tp, n_sp = lax.axis_size("tp"), lax.axis_size("sp")
    sharers = 2 * HEAD // keyval_first.shape[1]
    if sharers > 1:
        groups = [list(range(low, low + sharers)) for low in range(0, n_tp, sharers)]
        keyval_first, keyval_second = (
            lax.all_gather(w, "tp", axis=1, tiled=True, axis_index_groups=groups)
            for w in (keyval_first, keyval_second)
        )
    rows, width = target.shape
    lines = source.shape[0]
    block_rows = rows * n_tp
    columns = query_first.shape[1] // HEAD * block_rows
    n_chip = n_tp // 2
    span = width // PIECES
    dma = pltpu.SemaphoreType.DMA
    hbm = pl.BlockSpec(memory_space=pltpu.HBM)
    vmem = pl.BlockSpec(memory_space=pltpu.VMEM)

    def row(gain):
        return gain.reshape(1, width)

    line = pltpu.VMEM((1, width), F32)
    scratch = [
        *([line] * 4), pltpu.VMEM(conv_gate.shape, F32), pltpu.VMEM(conv_value.shape, F32),
        *([line] * 3),
        pltpu.VMEM(target.shape, BF16),
        pltpu.VMEM(source.shape, BF16),
        *(pltpu.VMEM(w.shape, BF16) for w in (
            query_first, keyval_first, out_first, w_gate.T, w_value.T, w_gate, w_value, w_down,
            query_second, keyval_second, out_second)),
        dma((20,)),
        pltpu.VMEM((3, PIECES, n_tp, rows, span), BF16),
        dma,
        dma((3, PIECES, n_chip)),
        pltpu.VMEM((n_tp, CHUNKS, lines // CHUNKS, width), BF16),
        dma,
        dma((2 * n_chip - 1, CHUNKS)),
        pltpu.VMEM((n_sp, HEAD, columns), BF16),
        dma((2,)),
        pltpu.VMEM((n_chip, 2 * lines, HEAD), BF16),
        pltpu.VMEM((n_chip, 2 * lines, HEAD), BF16),
        pltpu.VMEM((n_sp, n_chip, CHUNKS, 2, 2 * lines // CHUNKS, HEAD), BF16),
        dma,
        dma((n_sp - 1, n_chip, 2)),
        pltpu.VMEM((n_sp, 1, columns), F32),
        pltpu.VMEM((n_sp, 1, columns), F32),
        pltpu.VMEM((n_sp, HEAD, columns), F32),
        pltpu.VMEM((n_sp, HEAD, columns), BF16),
        pltpu.VMEM((n_sp, HEAD, columns), BF16),
        pltpu.VMEM((n_sp, 2, columns), F32),
        pltpu.VMEM((n_sp, 2, columns), F32),
        dma((2, n_sp + 1)),
        pltpu.VMEM((3, PIECES, 2, n_chip, rows, span), BF16),
        pltpu.VMEM((3, PIECES, n_chip, rows, span), BF16),
        pltpu.VMEM((3, PIECES, n_chip, rows, span), BF16),
        pltpu.VMEM((3, PIECES, n_chip, rows, span), BF16),
        dma((2,)),
        dma((3, PIECES)),
        dma((3, PIECES, n_chip - 1)),
        pltpu.VMEM((2, width), BF16),
        pltpu.VMEM((2, width), BF16),
        dma((2,)),
        pltpu.VMEM((rows, width), F32),
        pltpu.VMEM((HEAD, columns), BF16),
        pltpu.VMEM((2, columns), F32),
        dma((2, 2)),
    ]

    def kernel(*refs):
        decoder_kernel(n_tp, n_sp, *refs)

    return pl.pallas_call(
        kernel,
        out_shape=pltpu.VMEM((rows, width), F32),
        in_specs=[hbm] * 20,
        out_specs=vmem,
        scratch_shapes=scratch,
        compiler_params=pltpu.CompilerParams(
            collective_id=0, has_side_effects=True, vmem_limit_bytes=60_000_000
        ),
        name="decoder",
    )(
        target, source, row(source_gain), row(pre_first), query_first, keyval_first, out_first,
        row(post_first), row(ffn_pre), w_gate.T, w_value.T, conv_gate, conv_value, w_down,
        row(ffn_post), row(pre_second), query_second, keyval_second, out_second, row(post_second),
    )


def solution(mesh):
    rows = P(("grp", "sp", "tp"), None)
    by_column, by_row = P(None, "tp"), P("tp", None)
    placed = (
        rows, rows, P(), P(), by_column, by_column, by_row, P(), P(), by_column, by_column,
        by_column, by_column, by_row, P(), P(), by_column, by_column, by_row, P(),
    )
    return jax.shard_map(
        per_device, mesh=mesh, in_specs=placed, out_specs=rows, check_vma=False
    )
```

```python
import math

import jax
import jax.numpy as jnp
from jax import lax
from jax.experimental import pallas as pl
from jax.experimental.pallas import tpu as pltpu
from jax.sharding import PartitionSpec as P

HEAD = 128
CHUNKS = 4
PIECES = 2
EXP_SCALE = HEAD ** (-0.5) * math.log2(math.e)
F32, BF16 = jnp.float32, jnp.bfloat16
MESH = pl.DeviceIdType.MESH


def normed(values, gain):
    widened = values.astype(F32)
    return widened * lax.rsqrt(jnp.mean(widened * widened, axis=-1, keepdims=True) + 1e-06) * gain


SC = jax.named_scope


def times(start, stop, body):
    if stop - start <= 4:
        for index in range(start, stop):
            body(index)
    else:

        @pl.loop(start, stop)
        def _(index):
            body(index)


def dot(left, right):
    return jnp.dot(left, right, preferred_element_type=F32)


def decoder_kernel(
    n_tp,
    n_sp,
    target_h,
    source_h,
    source_gain_h,
    pre_first_h,
    query_first_h,
    keyval_first_h,
    out_first_h,
    post_first_h,
    ffn_pre_h,
    gate_h,
    value_h,
    conv_gate_h,
    conv_value_h,
    down_h,
    ffn_post_h,
    pre_second_h,
    query_second_h,
    keyval_second_h,
    out_second_h,
    post_second_h,
    decoded,
    source_gain,
    pre_first,
    post_first,
    ffn_pre,
    conv_gate,
    conv_value,
    ffn_post,
    pre_second,
    post_second,
    target_v,
    source_v,
    query_first,
    keyval_first,
    out_first,
    gate_t,
    value_t,
    w_gate,
    w_value,
    w_down,
    query_second,
    keyval_second,
    out_second,
    local_sem,
    hidden,
    hidden_send,
    hidden_recv,
    src,
    src_send,
    src_recv,
    q_slots,
    q_sem,
    k_first,
    v_first,
    kv_second,
    kv_send,
    kv_recv,
    run_max,
    run_sum,
    run_out,
    mix_send,
    mix_recv,
    stat_send,
    stat_recv,
    mix_sem,
    part,
    pair_recv,
    pair_sum,
    part_recv,
    part_send,
    pair_sem,
    part_sem,
    halo_send,
    halo_recv,
    halo_sem,
    stream,
    relay_mix,
    relay_stat,
    relay_sem,
):
    me = lax.axis_index("tp")
    z = lax.axis_index("sp")
    sib = me + 1 - 2 * lax.rem(me, 2)
    core, chip = lax.rem(me, 2), me // 2
    n_chip = n_tp // 2
    rows = target_v.shape[0]
    width = target_v.shape[1]
    span = width // PIECES
    chunk = src.shape[2]
    block_rows = rows * n_tp

    def tp_at(distance):
        return lax.rem(me + distance, n_tp)

    def sp_at(distance):
        return lax.rem(z + distance, n_sp)

    def to_tp(source, dest, send, recv, device):
        return pltpu.make_async_remote_copy(
            src_ref=source, dst_ref=dest, send_sem=send, recv_sem=recv,
            device_id={"tp": device}, device_id_type=MESH,
        )

    def to_sp(source, dest, send, recv, device):
        return pltpu.make_async_remote_copy(
            src_ref=source, dst_ref=dest, send_sem=send, recv_sem=recv,
            device_id={"sp": device}, device_id_type=MESH,
        )

    pairs = [
        (target_h, target_v),
        (source_h, source_v),
        (query_first_h, query_first),
        (keyval_first_h, keyval_first),
        (keyval_second_h, keyval_second),
        (out_first_h, out_first),
        (gate_h, gate_t),
        (value_h, value_t),
        (down_h, w_down),
        (query_second_h, query_second),
        (out_second_h, out_second),
    ]
    loads = [
        pltpu.make_async_copy(a, b, local_sem.at[i])
        for i, (a, b) in enumerate(pairs)
    ]
    vectors = {
        name: pltpu.make_async_copy(a, b, local_sem.at[len(pairs) + i])
        for i, (name, a, b) in enumerate([
            ("pre_first", pre_first_h, pre_first),
            ("source_gain", source_gain_h, source_gain),
            ("post_first", post_first_h, post_first),
            ("ffn_pre", ffn_pre_h, ffn_pre),
            ("conv_gate", conv_gate_h, conv_gate),
            ("conv_value", conv_value_h, conv_value),
            ("ffn_post", ffn_post_h, ffn_post),
            ("pre_second", pre_second_h, pre_second),
            ("post_second", post_second_h, post_second),
        ])
    }
    loads[0].start()
    vectors["pre_first"].start()
    vectors["source_gain"].start()
    for load in loads[1:]:
        load.start()
    for name in list(vectors)[2:]:
        vectors[name].start()

    barrier = pltpu.get_barrier_semaphore()
    for distance in range(1, n_tp):
        pl.semaphore_signal(barrier, inc=1, device_id={"tp": tp_at(distance)}, device_id_type=MESH)
    for distance in range(1, n_sp):
        pl.semaphore_signal(barrier, inc=1, device_id={"sp": sp_at(distance)}, device_id_type=MESH)
    last_tp = n_tp - 1

    @pl.when(jnp.logical_and(z > 0, me < last_tp))
    def _():
        pl.semaphore_signal(
            barrier, inc=1, device_id={"sp": z - 1, "tp": last_tp}, device_id_type=MESH
        )

    gives_halo = jnp.logical_and(me == last_tp, z < n_sp - 1)
    with SC("barrier"):
        pl.semaphore_wait(barrier, n_tp - 1 + n_sp - 1 + jnp.where(gives_halo, n_tp - 1, 0))

    def hidden_copy(phase, piece, slot, device, index=0):
        return to_tp(
            hidden.at[phase, piece, slot], hidden.at[phase, piece, slot],
            hidden_send, hidden_recv.at[phase, piece, index], device,
        )

    def gather_start(phase, value):
        for piece in range(PIECES):
            hidden[phase, piece, me] = value[:, piece * span : (piece + 1) * span].astype(BF16)
            for d in range(1, n_chip):
                hidden_copy(phase, piece, me, tp_at(2 * d), n_chip - d).start()
            hidden_copy(phase, piece, me, sib).start()

    def gather_times(phase, weights, extra=None):
        totals = [None] * len(weights)
        for piece in range(PIECES + 1):
            if piece < PIECES:
                for d in range(1, n_chip):
                    slot = tp_at(2 * d)
                    hidden_copy(phase, piece, slot, sib, d).wait_recv()
                    hidden_copy(phase, piece, slot, sib).start()
            if piece == 0:
                continue
            ready = piece - 1
            both = hidden.at[phase, ready, pl.ds(0, n_chip)]
            pltpu.make_async_copy(both, both, hidden_recv.at[phase, ready, 0]).wait()
            whole = hidden[phase, ready]
            if rows % 16:
                whole = whole.astype(F32).reshape(block_rows, span).astype(BF16)
            else:
                whole = whole.reshape(block_rows, span)
            if extra is not None:
                if ready == 0:
                    rim = extra()
                whole = jnp.concatenate([whole, rim[:, ready * span : (ready + 1) * span]], axis=0)
            for index, weight in enumerate(weights):
                product = dot(whole, weight[ready * span : (ready + 1) * span, :])
                totals[index] = product if ready == 0 else totals[index] + product
        return totals

    def gather_drain(phase):
        for piece in range(PIECES):
            for _ in range(2 * n_chip - 1):
                hidden_copy(phase, piece, me, sib).wait_send()

    def pair_copy(phase, piece):
        return to_tp(
            part.at[phase, piece, 1 - core], pair_recv.at[phase, piece],
            part_send.at[0], pair_sem.at[phase, piece], sib,
        )

    def chip_copy(phase, piece, distance, slot, index):
        other = lax.rem(chip + distance, n_chip)
        return to_tp(
            pair_sum.at[phase, piece, other], part_recv.at[phase, piece, slot],
            part_send.at[1], part_sem.at[phase, piece, index], 2 * other + core,
        )

    def scatter_sum(phase, left, weight, between=None):
        for piece in range(PIECES):
            product = dot(left, weight[:, piece * span : (piece + 1) * span])
            product = product.reshape(n_chip, 2, rows, span)
            for parity in range(2):
                part[phase, piece, parity] = product[:, parity].astype(BF16)
            pair_copy(phase, piece).start()
        if between is not None:
            between()
        for piece in range(PIECES):
            pair_copy(phase, piece).wait_recv()
            mine = part[phase, piece, core].astype(F32)
            pair_sum[phase, piece] = (mine + pair_recv[phase, piece].astype(F32)).astype(BF16)
            for d in range(1, n_chip):
                chip_copy(phase, piece, d, chip, n_chip - d - 1).start()
        sums = []
        for piece in range(PIECES):
            total = pair_sum[phase, piece, chip].astype(F32)
            for d in range(1, n_chip):
                slot = lax.rem(chip + d, n_chip)
                chip_copy(phase, piece, d, slot, d - 1).wait_recv()
                total = total + part_recv[phase, piece, slot].astype(F32)
            sums.append(total)
        return jnp.concatenate(sums, axis=1)

    def sum_drain(phase):
        for piece in range(PIECES):
            pair_copy(phase, piece).wait_send()
            for d in range(1, n_chip):
                chip_copy(phase, piece, d, chip, d - 1).wait_send()

    def head_columns(queries):
        blocks = [
            queries[:, h : h + HEAD].T for h in range(0, queries.shape[1], HEAD)
        ]
        return jnp.concatenate(blocks, axis=1).astype(BF16)

    def head_rows(columns):
        blocks = [
            columns[:, c : c + block_rows].T for c in range(0, columns.shape[1], block_rows)
        ]
        return jnp.concatenate(blocks, axis=1).astype(BF16)

    loads[0].wait()
    vectors["pre_first"].wait()
    with SC("norm0"):
        gather_start(0, normed(target_v[...], pre_first[...]))

    def src_copy(slot, c, device, index):
        return to_tp(src.at[slot, c], src.at[slot, c], src_send, src_recv.at[index, c], device)

    loads[1].wait()
    vectors["source_gain"].wait()
    for c in range(CHUNKS):
        src[me, c] = normed(source_v[pl.ds(c * chunk, chunk)], source_gain[...]).astype(BF16)
        for d in range(1, n_chip):
            src_copy(me, c, tp_at(2 * d), n_chip - d).start()
        src_copy(me, c, sib, 0).start()

    def project_pair(block, c, mine, other, layers=(0, 1)):
        lines = jnp.concatenate([src[mine, c], src[other, c]], axis=0)
        place = pl.ds(c * 2 * chunk, 2 * chunk)
        if 0 in layers:
            first = dot(lines, keyval_first[...])
            k_first[block, place] = first[:, :HEAD].astype(BF16)
            v_first[block, place] = first[:, HEAD:].astype(BF16)
        if 1 in layers:
            second = dot(lines, keyval_second[...])
            kv_second[z, block, c, 0] = second[:, :HEAD].astype(BF16)
            kv_second[z, block, c, 1] = second[:, HEAD:].astype(BF16)

    def absorb(keys, values, queries, slot, fresh):
        absorb_scores(dot(keys, queries), values, slot, fresh)

    def absorb_scores(scores, values, slot, fresh):
        newest = jnp.max(scores, axis=0, keepdims=True)
        if not fresh:
            newest = jnp.maximum(newest, run_max[slot])
        weights = jnp.exp2((scores - newest) * EXP_SCALE)
        added = jnp.sum(weights, axis=0, keepdims=True)
        gathered = lax.dot_general(
            values, weights.astype(BF16), (((0,), (0,)), ((), ())), preferred_element_type=F32
        )
        if not fresh:
            rescale = jnp.exp2((run_max[slot] - newest) * EXP_SCALE)
            added = added + run_sum[slot] * rescale
            gathered = gathered + run_out[slot] * rescale
        run_max[slot] = newest
        run_sum[slot] = added
        run_out[slot] = gathered

    def absorb_block(block, fresh):
        @pl.loop(0, n_sp)
        def _(slot):
            absorb(k_first[block], v_first[block], q_slots[slot], slot, fresh)

    last = n_chip - 1
    lead = CHUNKS // 2

    def kv_copy(block, slot, c, peer, receiver):
        held = kv_second.at[slot, block, c]
        index = slot - jnp.where(slot > receiver, 1, 0)
        group = int(c >= (lead if block == 0 else CHUNKS - 1))
        return to_sp(held, held, kv_send, kv_recv.at[index, block, group], peer)

    def kv_wait(block, slot, chunks):
        edge = lead if block == 0 else CHUNKS - 1
        index = slot - jnp.where(slot > z, 1, 0)
        for group in range(2):
            count = sum(int(c >= edge) == group for c in chunks)
            if count:
                held = kv_second.at[slot, block, pl.ds(edge * group, count)]
                pltpu.make_async_copy(held, held, kv_recv.at[index, block, group]).wait()

    def kv_hop(block, hop, arrive=True, chunks=range(CHUNKS)):
        for step in (1, -1):
            slot = z - step * (hop - 1)
            peer = z + step

            @pl.when(jnp.logical_and(slot >= 0, slot < n_sp))
            def _():
                if arrive:
                    kv_wait(block, slot, chunks)

                @pl.when(jnp.logical_and(hop < n_sp, jnp.logical_and(peer >= 0, peer < n_sp)))
                def _():
                    for c in chunks:
                        kv_copy(block, slot, c, peer, peer).start()

    def kv_drain(block, hop):
        for step in (1, -1):
            slot = z - step * (hop - 1)
            peer = z + step
            inside = jnp.logical_and(slot >= 0, slot < n_sp)

            @pl.when(jnp.logical_and(inside, jnp.logical_and(peer >= 0, peer < n_sp)))
            def _():
                for c in range(CHUNKS):
                    kv_copy(block, slot, c, peer, peer).wait_send()

    def nearest(j):
        up = j + jnp.where(j >= z, 1, 0)
        down = n_sp - 1 - j
        down = down - jnp.where(down <= z, 1, 0)
        return jnp.where(2 * z < n_sp, up, down)

    def second_rows(slot, part):
        return kv_second[slot, :, :, part].reshape(n_chip * CHUNKS * 2 * chunk, HEAD)

    loads[3].wait()
    loads[4].wait()
    with SC("proj_own"):
        for c in range(CHUNKS):
            src_copy(sib, c, sib, 0).wait_recv()
            project_pair(0, c, me, sib)
    kv_hop(0, 1, False, range(CHUNKS // 2))
    loads[2].wait()
    with SC("qproj"):
        q_slots[z] = head_columns(gather_times(0, [query_first])[0])

    def q_copy(distance, slot):
        return to_sp(
            q_slots.at[z], q_slots.at[z] if slot is None else q_slots.at[slot],
            q_sem.at[0], q_sem.at[1], sp_at(distance),
        )

    for d in range(1, n_sp):
        q_copy(d, None).start()


    def near_chunk(d, c):
        near = tp_at(2 * d)
        src_copy(near, c, sib, d).wait_recv()
        src_copy(near, c, sib, n_chip - 1 + d).start()

    def far_chunk(d, c, layers=(0, 1)):
        far = lax.rem(sib + 2 * d, n_tp)
        src_copy(far, c, sib, n_chip - 1 + d).wait_recv()
        project_pair(d, c, tp_at(2 * d), far, layers)

    def absorb_chunks(low, high):
        place = slice(low * 2 * chunk, high * 2 * chunk)

        @pl.loop(0, n_sp)
        def _(slot):
            absorb(k_first[last, place], v_first[last, place], q_slots[slot], slot, False)

    def lead_chunks():
        for c in range(lead):
            near_chunk(last, c)
            far_chunk(last, c)

    if n_chip == 2:
        with SC("lead"):
            lead_chunks()
    with SC("qwait"):
        others = q_slots.at[pl.ds(0, n_sp - 1)]
        pltpu.make_async_copy(others, others, q_sem.at[1]).wait()
    kv_hop(0, 1, False, range(lead, CHUNKS))
    kv_hop(0, 2, True, range(lead))
    with SC("abs_own"):
        absorb_block(0, True)

    def far_absorb(d):
        for c in range(CHUNKS):
            near_chunk(d, c)
            far_chunk(d, c)
        absorb_block(d, False)

    times(1, last, far_absorb)
    if n_chip > 2:
        lead_chunks()
    kv_hop(last, 1, False, range(lead))
    for c in range(lead, CHUNKS - 1):
        with SC("near"):
            near_chunk(last, c)
        with SC("abs_early"):
            absorb_chunks(0 if c == lead else c - 1, c)
        with SC("far"):
            far_chunk(last, c)
        kv_hop(last, 1, False, (c,))
    with SC("abs_early2"):
        absorb_chunks(CHUNKS - 2, CHUNKS - 1)
    with SC("near_last"):
        near_chunk(last, CHUNKS - 1)
    with SC("far_last"):
        far_chunk(last, CHUNKS - 1, (0,))
    early = (CHUNKS - 1) * 2 * chunk

    def mix_copies(peer, slot):
        return [
            to_sp(sent.at[peer], got.at[slot], mix_sem.at[index, n_sp], mix_sem.at[index, slot], peer)
            for index, (sent, got) in enumerate(((mix_send, mix_recv), (stat_send, stat_recv)))
        ]

    def finish_slot(slot):
        absorb(k_first[last, early:], v_first[last, early:], q_slots[slot], slot, False)

    def pack(peer):
        total = run_sum[peer]
        mix_send[peer] = (run_out[peer] / total).astype(BF16)
        stat_send[peer] = jnp.concatenate([run_max[peer], total], axis=0)

    def finish_and_send(peer):
        finish_slot(peer)
        pack(peer)
        for copy in mix_copies(peer, z):
            copy.start()

    relayed = n_sp > 2
    end = n_sp - 1
    gives, merges, takes = z == 0, z == 1, z == end

    def relay_copies():
        return [
            to_sp(sent.at[end], got, relay_sem.at[index, 0], relay_sem.at[index, 1], 1)
            for index, (sent, got) in enumerate(((mix_send, relay_mix), (stat_send, relay_stat)))
        ]

    def mix_order(j):
        return jnp.where(
            merges, jnp.where(j == n_sp - 2, end, nearest(n_sp - 2 - j - 1)), nearest(n_sp - 2 - j)
        )

    if relayed:

        @pl.loop(0, n_sp - 1)
        def _(j):
            peer = mix_order(j)
            finish_slot(peer)

            @pl.when(jnp.logical_not(jnp.logical_and(merges, peer == end)))
            def _():
                pack(peer)

                @pl.when(jnp.logical_and(gives, peer == end))
                def _():
                    for copy in relay_copies():
                        copy.start()

                @pl.when(jnp.logical_not(jnp.logical_and(gives, peer == end)))
                def _():
                    for copy in mix_copies(peer, z):
                        copy.start()

    else:

        @pl.loop(0, n_sp - 1)
        def _(j):
            finish_and_send(nearest(n_sp - 2 - j))

    with SC("finish_me"):
        finish_slot(z)
        project_pair(last, CHUNKS - 1, tp_at(2 * last), lax.rem(sib + 2 * last, n_tp), (1,))
    with SC("transpose"):
        for load in loads[5:]:
            load.wait()
        for name in list(vectors)[2:]:
            vectors[name].wait()
        stripe = 2 * HEAD

        @pl.loop(0, width // stripe)
        def _(index):
            place = pl.ds(pl.multiple_of(index * stripe, stripe), stripe)
            w_gate[place, :] = gate_t[:, place].T
            w_value[place, :] = value_t[:, place].T

    def merge_into(slot, values, newest, count):
        top = jnp.maximum(newest, run_max[slot])
        rescale = jnp.exp2((run_max[slot] - top) * EXP_SCALE)
        share = jnp.exp2((newest - top) * EXP_SCALE) * count
        run_max[slot] = top
        run_sum[slot] = run_sum[slot] * rescale + share
        run_out[slot] = run_out[slot] * rescale + values.astype(F32) * share

    def merge(slot):
        for copy in mix_copies(slot, slot):
            copy.wait_recv()
        merge_into(z, mix_recv[slot], stat_recv[slot, 0:1], stat_recv[slot, 1:2])

    if relayed:
        with SC("relay"):

            @pl.when(merges)
            def _():
                for copy in relay_copies():
                    copy.wait_recv()
                merge_into(end, relay_mix[...], relay_stat[0:1], relay_stat[1:2])
                pack(end)
                for copy in mix_copies(end, z):
                    copy.start()

    with SC("mixwait"):
        @pl.loop(0, n_sp - 1)
        def _(j):
            slot = nearest(j)

            @pl.when(jnp.logical_not(jnp.logical_and(takes, slot == 0) if relayed else z < 0))
            def _():
                merge(slot)

    def relays_first():
        kv_hop(last, 1, False, (CHUNKS - 1,))
        for block in range(1, last):
            kv_hop(block, 1, False)
        kv_hop(0, 2, True, range(lead, CHUNKS))
        kv_hop(last, 2, True, range(CHUNKS - 1))
    with SC("rs0"):
        mixed = scatter_sum(0, head_rows(run_out[z] / run_sum[z]), out_first, relays_first)
    after_first = target_v[...].astype(F32) + normed(mixed, post_first[...])
    stream[...] = after_first

    def halo_copy(device):
        return pltpu.make_async_remote_copy(
            src_ref=halo_send, dst_ref=halo_recv, send_sem=halo_sem.at[0],
            recv_sem=halo_sem.at[1], device_id=device, device_id_type=MESH,
        )

    ffn_input = normed(after_first, ffn_pre[...])

    @pl.when(gives_halo)
    def _():
        halo_send[...] = ffn_input[rows - 2 :].astype(BF16)
        for t in range(n_tp):
            halo_copy({"sp": z + 1, "tp": t}).start()

    gather_start(1, ffn_input)
    with SC("kv_b"):
        for block in range(1, last):
            kv_hop(block, 2)
        kv_hop(0, 3, True, range(lead))
        kv_hop(last, 2, True, (CHUNKS - 1,))

    def halo_rows():
        @pl.when(z > 0)
        def _():
            halo_copy({"sp": z, "tp": sib}).wait_recv()

        zeros = jnp.zeros((14, width), F32)
        return jnp.concatenate([halo_recv[...].astype(F32), zeros], axis=0).astype(BF16)

    with SC("ag1_up"):
        up_gate, up_value = (
            up.astype(BF16) for up in gather_times(1, [w_gate, w_value], halo_rows)
        )

    def causal_mix(up_rows, taps):
        here = up_rows[:block_rows].astype(F32)
        rim = jnp.where(z > 0, up_rows[block_rows:].astype(F32), 0.0)
        row = lax.broadcasted_iota(jnp.int32, here.shape, 0)
        before = jnp.where(row == 0, rim[1:2], pltpu.roll(here, 1, 0))
        earlier = jnp.where(
            row == 0, rim[0:1], jnp.where(row == 1, rim[1:2], pltpu.roll(here, 2, 0))
        )
        return taps[0:1] * earlier + taps[1:2] * before + taps[2:3] * here

    with SC("gated"):
        gated = (
            jax.nn.gelu(causal_mix(up_gate, conv_gate[...]), approximate=True)
            * causal_mix(up_value, conv_value[...])
        ).astype(BF16)
    def relays_third():
        kv_hop(0, 3, True, range(lead, CHUNKS))
        kv_hop(last, 3, True, range(CHUNKS - 1))
    with SC("rs1"):
        ffn_sum = scatter_sum(1, gated, w_down, relays_third)
    after_ffn = stream[...] + normed(ffn_sum, ffn_post[...])
    stream[...] = after_ffn

    gather_start(2, normed(after_ffn, pre_second[...]))
    with SC("kv_d"):
        for block in range(1, last):
            kv_hop(block, 3)
        kv_hop(last, 3, True, (CHUNKS - 1,))
    with SC("ag2_q"):
        queries = head_columns(gather_times(2, [query_second])[0])
        for d in range(1, n_sp):
            q_copy(d, None).wait_send()
        q_slots[z] = queries

    def kv_rest():
        @pl.loop(4, max(n_sp, 4) + 1)
        def _(hop):
            for block in range(n_chip):
                kv_hop(block, hop)

    def absorb_second(j):
        slot = nearest(j)
        absorb(second_rows(slot, 0), second_rows(slot, 1), q_slots[z], 0, False)

    with SC("attn2"):
        if n_sp > 4:
            absorb(second_rows(z, 0), second_rows(z, 1), q_slots[z], 0, True)
            kv_rest()
            times(0, n_sp - 1, absorb_second)
        else:
            slots = [z] + [nearest(j) for j in range(n_sp - 1)]
            scores = dot(second_rows(z, 0), q_slots[z])
            for index, slot in enumerate(slots):
                if index == n_sp - 2:
                    kv_rest()
                if index < n_sp - 1:
                    ahead = dot(second_rows(slots[index + 1], 0), q_slots[z])
                absorb_scores(scores, second_rows(slot, 1), 0, index == 0)
                scores = ahead

    with SC("rs2"):
        mixed = scatter_sum(2, head_rows(run_out[0] / run_sum[0]), out_second)
    decoded[...] = stream[...] + normed(mixed, post_second[...])

    for phase in range(3):
        gather_drain(phase)
        sum_drain(phase)
    for c in range(CHUNKS):
        for _ in range(n_chip):
            src_copy(me, c, sib, 0).wait_send()
        for d in range(1, n_chip):
            src_copy(me, c, sib, 1).wait_send()

    def drain(d):
        for block in range(n_chip):
            kv_drain(block, d)
        relay = jnp.logical_and(gives, sp_at(d) == end) if relayed else z < 0

        @pl.when(jnp.logical_not(relay))
        def _():
            for copy in mix_copies(sp_at(d), z):
                copy.wait_send()

    times(1, n_sp, drain)
    if relayed:

        @pl.when(gives)
        def _():
            for copy in relay_copies():
                copy.wait_send()

    @pl.when(gives_halo)
    def _():
        for t in range(n_tp):
            halo_copy({"sp": z, "tp": sib}).wait_send()


def per_device(*arrays):
    (target, source, source_gain, pre_first, query_first, keyval_first, out_first, post_first,
     ffn_pre, w_gate, w_value, conv_gate, conv_value, w_down, ffn_post, pre_second,
     query_second, keyval_second, out_second, post_second) = arrays
    n_tp, n_sp = lax.axis_size("tp"), lax.axis_size("sp")
    sharers = 2 * HEAD // keyval_first.shape[1]
    if sharers > 1:
        groups = [list(range(low, low + sharers)) for low in range(0, n_tp, sharers)]
        keyval_first, keyval_second = (
            lax.all_gather(w, "tp", axis=1, tiled=True, axis_index_groups=groups)
            for w in (keyval_first, keyval_second)
        )
    rows, width = target.shape
    lines = source.shape[0]
    block_rows = rows * n_tp
    columns = query_first.shape[1] // HEAD * block_rows
    n_chip = n_tp // 2
    span = width // PIECES
    dma = pltpu.SemaphoreType.DMA
    hbm = pl.BlockSpec(memory_space=pltpu.HBM)
    vmem = pl.BlockSpec(memory_space=pltpu.VMEM)

    def row(gain):
        return gain.reshape(1, width)

    line = pltpu.VMEM((1, width), F32)
    scratch = [
        *([line] * 4), pltpu.VMEM(conv_gate.shape, F32), pltpu.VMEM(conv_value.shape, F32),
        *([line] * 3),
        pltpu.VMEM(target.shape, BF16),
        pltpu.VMEM(source.shape, BF16),
        *(pltpu.VMEM(w.shape, BF16) for w in (
            query_first, keyval_first, out_first, w_gate.T, w_value.T, w_gate, w_value, w_down,
            query_second, keyval_second, out_second)),
        dma((20,)),
        pltpu.VMEM((3, PIECES, n_tp, rows, span), BF16),
        dma,
        dma((3, PIECES, n_chip)),
        pltpu.VMEM((n_tp, CHUNKS, lines // CHUNKS, width), BF16),
        dma,
        dma((2 * n_chip - 1, CHUNKS)),
        pltpu.VMEM((n_sp, HEAD, columns), BF16),
        dma((2,)),
        pltpu.VMEM((n_chip, 2 * lines, HEAD), BF16),
        pltpu.VMEM((n_chip, 2 * lines, HEAD), BF16),
        pltpu.VMEM((n_sp, n_chip, CHUNKS, 2, 2 * lines // CHUNKS, HEAD), BF16),
        dma,
        dma((n_sp - 1, n_chip, 2)),
        pltpu.VMEM((n_sp, 1, columns), F32),
        pltpu.VMEM((n_sp, 1, columns), F32),
        pltpu.VMEM((n_sp, HEAD, columns), F32),
        pltpu.VMEM((n_sp, HEAD, columns), BF16),
        pltpu.VMEM((n_sp, HEAD, columns), BF16),
        pltpu.VMEM((n_sp, 2, columns), F32),
        pltpu.VMEM((n_sp, 2, columns), F32),
        dma((2, n_sp + 1)),
        pltpu.VMEM((3, PIECES, 2, n_chip, rows, span), BF16),
        pltpu.VMEM((3, PIECES, n_chip, rows, span), BF16),
        pltpu.VMEM((3, PIECES, n_chip, rows, span), BF16),
        pltpu.VMEM((3, PIECES, n_chip, rows, span), BF16),
        dma((2,)),
        dma((3, PIECES)),
        dma((3, PIECES, n_chip - 1)),
        pltpu.VMEM((2, width), BF16),
        pltpu.VMEM((2, width), BF16),
        dma((2,)),
        pltpu.VMEM((rows, width), F32),
        pltpu.VMEM((HEAD, columns), BF16),
        pltpu.VMEM((2, columns), F32),
        dma((2, 2)),
    ]

    def kernel(*refs):
        decoder_kernel(n_tp, n_sp, *refs)

    return pl.pallas_call(
        kernel,
        out_shape=pltpu.VMEM((rows, width), F32),
        in_specs=[hbm] * 20,
        out_specs=vmem,
        scratch_shapes=scratch,
        compiler_params=pltpu.CompilerParams(
            collective_id=0, has_side_effects=True, vmem_limit_bytes=60_000_000,
        ),
        name="decoder",
    )(
        target, source, row(source_gain), row(pre_first), query_first, keyval_first, out_first,
        row(post_first), row(ffn_pre), w_gate.T, w_value.T, conv_gate, conv_value, w_down,
        row(ffn_post), row(pre_second), query_second, keyval_second, out_second, row(post_second),
    )


def solution(mesh):
    rows = P(("grp", "sp", "tp"), None)
    by_column, by_row = P(None, "tp"), P("tp", None)
    placed = (
        rows, rows, P(), P(), by_column, by_column, by_row, P(), P(), by_column, by_column,
        by_column, by_column, by_row, P(), P(), by_column, by_column, by_row, P(),
    )
    return jax.shard_map(
        per_device, mesh=mesh, in_specs=placed, out_specs=rows, check_vma=False
    )
```
